32 devices in a mesh: ep: 8 (over z, y), tp: 4 (over x, core).
Axes of the slice: x: 2, y: 2, z: 4, core: 2. Of those that a mesh axis runs over, the one named last changes fastest.
Arguments:
- tokens: bfloat16 [128, 4096], P(None, 'ep'), may hold values from -80 to 80
- mix_gain: bfloat16 [4096], P('ep'), may hold values from 0.099609375 to 1.8984375
- w_query: bfloat16 [4096, 1024], P('ep', 'tp'), may hold values from -0.09375 to 0.09375
- w_key: bfloat16 [4096, 1024], P('ep', 'tp'), may hold values from -0.09375 to 0.09375
- w_value: bfloat16 [4096, 2048], P('ep', 'tp'), may hold values from -0.09375 to 0.09375
- w_outgate: bfloat16 [4096, 2048], P('ep', 'tp'), may hold values from -0.09375 to 0.09375
- w_igate: bfloat16 [4096, 16], P('ep', 'tp'), may hold values from -0.09375 to 0.09375
- w_fgate: bfloat16 [4096, 16], P('ep', 'tp'), may hold values from -0.09375 to 0.09375
- igate_bias: float32 [16], P('tp'), may hold values from -3 to 3
- fgate_bias: float32 [16], P('tp'), may hold values from -1 to 3
- head_gain: bfloat16 [2048], P('tp'), may hold values from 0.099609375 to 1.8984375
- w_mixout: bfloat16 [2048, 4096], P('tp', 'ep'), may hold values from -0.125 to 0.125
- state_matrix: float32 [128, 16, 64, 128], P('ep', 'tp'), may hold values from -3 to 3
- state_norm: float32 [128, 16, 64], P('ep', 'tp'), may hold values from -3 to 3
- state_max: float32 [128, 16], P('ep', 'tp'), may hold values from -3 to 3
- ffn_gain: bfloat16 [4096], P('ep'), may hold values from 0.099609375 to 1.8984375
- dense_mix: bfloat16 [4096], P('ep'), may hold values from -0.09375 to 0.09375
- w_dense_gate: bfloat16 [4096, 1024], P('ep', 'tp'), may hold values from -0.09375 to 0.09375
- w_dense_up: bfloat16 [4096, 1024], P('ep', 'tp'), may hold values from -0.09375 to 0.09375
- w_dense_down: bfloat16 [1024, 4096], P('tp', 'ep'), may hold values from -0.1875 to 0.1875
- routes: int32 [128, 4], replicated, may hold values from 0 to 7, all different within a row; in each aligned block of 16 rows (0 to 15, 16 to 31, ...) at most 16 rows name the same one
- route_weights: float32 [128, 4], replicated, may hold values from 0.2 to 1.5
- w_exp_gate: bfloat16 [8, 4096, 1024], P('ep', None, 'tp'), may hold values from -0.09375 to 0.09375
- w_exp_up: bfloat16 [8, 4096, 1024], P('ep', None, 'tp'), may hold values from -0.09375 to 0.09375
- w_exp_down: bfloat16 [8, 1024, 4096], P('ep', 'tp'), may hold values from -0.1875 to 0.1875
Outputs:
- layer_out: bfloat16 [128, 4096], P(None, 'ep')
- new_matrix: float32 [128, 16, 64, 128], P('ep', 'tp')
- new_norm: float32 [128, 16, 64], P('ep', 'tp')
- new_max: float32 [128, 16], P('ep', 'tp')
The draws below stay inside these ranges and needn't reach their ends.
Inputs may be any that keep to these rules, and one draw needn't show every extreme that they name: `routes`: each row names 4 different experts. In the rows of one device (aligned blocks of 16 rows) no expert is named by more than 16 rows, a bound that some block reaches.
All inputs are finite; a program needn't handle non-finite values.
Results may differ from the reference program's by a relative error of at most 0.012.
Values may be sent and summed in bfloat16 or wider, within the bound.
A program may use at most 128 MiB of HBM per device.

```python
import math
import jax
import jax.numpy as jnp
import numpy as np
from jax import lax

D = 4096
H = 16
DK = 64
DV = 128
FE = 1024
FS = 1024
TOPK = 4
SEQ_DEV = 16
HQK = 1024
HV = 2048
EXPERTS = 8
BATCH = 128
CAP = 16
UNIT_GROUP = 256
N_EP = 8
N_TP = 4


def draw_tokens(key, part):
    base_key, scale_key, column_key = jax.random.split(key, 3)
    noise = jnp.clip(jax.random.normal(base_key, (BATCH, D), jnp.float32), -5.0, 5.0)
    row_scale = jnp.exp(jax.random.uniform(scale_key, (BATCH, 1), jnp.float32, math.log(0.4), math.log(2.5)))
    col_scale = 3.0 ** (jnp.arange(D, dtype=jnp.float32) / D) * jnp.exp(jax.random.uniform(column_key, (D,), jnp.float32, -0.35, 0.35))
    return (noise * row_scale * col_scale[None, :]).astype(jnp.bfloat16)


def level_of(rng, extent, cuts, least, top_value):
    loudness = 1.0
    for axis_at, blocks in cuts:
        steps = jax.random.uniform(jax.random.fold_in(jax.random.fold_in(rng, 6), axis_at), (blocks,), jnp.float32, least / len(cuts), top_value / len(cuts))
        loudness = loudness * jnp.repeat(jnp.exp(steps), extent[axis_at] // blocks).reshape((-1,) + (1,) * (len(extent) - 1 - axis_at))
    return loudness


def deal_out(rng, own, number, rows, amount, top, limit, lean):
    sequence = jax.random.permutation(rng, amount)
    heavy_load, common = load_shares(amount, rows * top, limit, lean, True), load_shares(amount, rows * top, limit, lean, False)
    places = jnp.arange(amount)

    def named(sizes, offset_by):
        used = int((sizes > 0).sum())
        fixed = max(1, used // 4)
        passed = fixed + (places - fixed + offset_by * (used - fixed)) % max(1, amount - fixed)
        return jnp.zeros((amount,), jnp.int32).at[sequence[jnp.where(places < fixed, places, passed)]].set(jnp.asarray(sizes, jnp.int32))

    sizes = jnp.where(number % 4 == 0, named(heavy_load, number // 4), named(common, number - number // 4 - 1))
    mixed = jax.random.permutation(jax.random.fold_in(own, 3), amount)
    source_of, receiver = mixed[0:amount // 2 * 2:2], mixed[1:amount // 2 * 2:2]
    room = jnp.minimum(sizes[source_of] - 1, limit - sizes[receiver]) // 2
    room = jnp.where((source_of == sequence[0]) | (receiver == sequence[0]) | (sizes[receiver] == 0), 0, jnp.maximum(room, 0))
    passed = jax.random.randint(jax.random.fold_in(own, 4), (amount // 2,), 0, 1 << 20) % (room + 1)
    sizes = sizes.at[source_of].add(-passed).at[receiver].add(passed)
    labels = jnp.searchsorted(jnp.cumsum(sizes), jnp.arange(rows * top), side="right").astype(jnp.int32)
    table = labels.reshape(top, rows).T
    table = table[jax.random.permutation(jax.random.fold_in(own, 1), rows)]
    offset_by = jax.random.randint(jax.random.fold_in(own, 2), (rows, 1), 0, top)
    return jnp.take_along_axis(table, (jnp.arange(top)[None, :] + offset_by) % top, axis=1)


def load_shares(count, total, bound, lean, full):
    weights = [(1 << 20) // math.isqrt(grade ** lean) + 1 for grade in range(1, count + 1)]
    largest = bound if full else min(bound, max(-(-total // count), total * weights[0] // sum(weights)))
    least = 1 if total - largest >= count - 1 else 0
    given, spare = [largest] + [least] * (count - 1), total - largest - least * (count - 1)
    while spare > 0:
        candidates = [i for i in range(1, count) if given[i] < largest] or [i for i in range(1, count) if given[i] < bound]
        whole, remaining = sum([weights[i] for i in candidates]), spare
        for i in candidates:
            extra = min(bound - given[i], max(1, remaining * weights[i] // whole), spare)
            given[i] = given[i] + extra
            spare = spare - extra
    return np.array(given)


def scatter_about(stream_key, shape, scale, reach, pieces=(), kind=jnp.bfloat16):
    array = scale * jax.random.normal(stream_key, shape, jnp.float32)
    if pieces:
        array = array * level_of(stream_key, shape, pieces, -0.22, 0.18)
    return jnp.clip(array, -reach, reach).astype(kind)


def setup_inputs(seed: int = 0) -> dict:
    keys = jax.random.split(jax.random.key(seed), 26)
    tokens = draw_tokens(jax.random.fold_in(keys[25], 71), 0)
    mix_gain = jnp.clip(1.0 + 0.18 * jax.random.normal(keys[1], (D,), jnp.float32), 0.099609375, 1.8984375).astype(jnp.bfloat16)
    w_query = scatter_about(keys[2], (D, HQK), D ** -0.5, 0.09375, ((0, 8), (1, 4)))
    w_key = scatter_about(keys[3], (D, HQK), D ** -0.5, 0.09375, ((0, 8), (1, 4)))
    w_value = scatter_about(keys[4], (D, HV), D ** -0.5, 0.09375, ((0, 8), (1, 4)))
    w_outgate = scatter_about(keys[5], (D, HV), D ** -0.5, 0.09375, ((0, 8), (1, 4)))
    w_igate = scatter_about(keys[6], (D, H), D ** -0.5, 0.09375, ((0, 8), (1, 4)))
    w_fgate = scatter_about(keys[7], (D, H), D ** -0.5, 0.09375, ((0, 8), (1, 4)))
    igate_bias = scatter_about(keys[8], (H,), 1.0, 3.0, ((0, 4),), jnp.float32)
    fgate_bias = jnp.clip(-1.0 + 4.0 * jax.random.uniform(keys[9], (H,), jnp.float32) ** level_of(keys[9], (H,), ((0, 4),), -0.2, 0.2), -1.0, 3.0)
    head_gain = jnp.clip(1.0 + 0.18 * jax.random.normal(keys[10], (HV,), jnp.float32), 0.099609375, 1.8984375).astype(jnp.bfloat16)
    w_mixout = scatter_about(keys[11], (HV, D), HV ** -0.5, 0.125, ((0, 4), (1, 8)))
    state_matrix = scatter_about(keys[12], (BATCH, H, DK, DV), 0.5, 3.0, ((0, 8), (1, 4)), jnp.float32)
    state_norm = scatter_about(keys[13], (BATCH, H, DK), 0.5, 3.0, ((0, 8), (1, 4)), jnp.float32)
    state_max = scatter_about(keys[14], (BATCH, H), 1.0, 3.0, ((0, 8), (1, 4)), jnp.float32)
    ffn_gain = jnp.clip(1.0 + 0.18 * jax.random.normal(keys[15], (D,), jnp.float32), 0.099609375, 1.8984375).astype(jnp.bfloat16)
    dense_mix = scatter_about(keys[16], (D,), D ** -0.5, 0.09375, ((0, 8),))
    w_dense_gate = scatter_about(keys[17], (D, FS), D ** -0.5, 0.09375, ((0, 8), (1, 4)))
    w_dense_up = scatter_about(keys[18], (D, FS), D ** -0.5, 0.09375, ((0, 8), (1, 4)))
    w_dense_down = scatter_about(keys[19], (FS, D), FS ** -0.5, 0.1875, ((0, 4), (1, 8)))
    routes_keys = jax.random.split(jax.random.fold_in(keys[20], 1), BATCH // SEQ_DEV)
    routes_turns = jax.random.permutation(jax.random.fold_in(keys[20], 3), BATCH // SEQ_DEV)
    routes = jax.vmap(lambda own, number: deal_out(jax.random.fold_in(keys[20], 2), own, number, SEQ_DEV, EXPERTS, TOPK, CAP, 2))(routes_keys, routes_turns).reshape((BATCH, TOPK))
    route_weights = jnp.clip(jnp.exp(jax.random.uniform(keys[21], (BATCH, TOPK), jnp.float32, math.log(0.2), math.log(1.5))), 0.2, 1.5)
    w_exp_gate = scatter_about(keys[22], (EXPERTS, D, FE), D ** -0.5, 0.09375, ((0, 8), (2, 4)))
    w_exp_up = scatter_about(keys[23], (EXPERTS, D, FE), D ** -0.5, 0.09375, ((0, 8), (2, 4)))
    w_exp_down = scatter_about(keys[24], (EXPERTS, FE, D), FE ** -0.5, 0.1875, ((0, 8), (1, 4)))
    return dict(tokens=tokens, mix_gain=mix_gain, w_query=w_query, w_key=w_key, w_value=w_value, w_outgate=w_outgate, w_igate=w_igate, w_fgate=w_fgate, igate_bias=igate_bias, fgate_bias=fgate_bias, head_gain=head_gain, w_mixout=w_mixout, state_matrix=state_matrix, state_norm=state_norm, state_max=state_max, ffn_gain=ffn_gain, dense_mix=dense_mix, w_dense_gate=w_dense_gate, w_dense_up=w_dense_up, w_dense_down=w_dense_down, routes=routes, route_weights=route_weights, w_exp_gate=w_exp_gate, w_exp_up=w_exp_up, w_exp_down=w_exp_down)


EPSILON = 1e-06
SOFT_CAP = 15.0

def gate_logs(in_pre, forget_pre, igate_bias, fgate_bias):
    in_log = SOFT_CAP * jnp.tanh((in_pre + igate_bias) / SOFT_CAP)
    forget_log = jax.nn.log_sigmoid(SOFT_CAP * jnp.tanh((forget_pre + fgate_bias) / SOFT_CAP))
    return (in_log, forget_log)

def recurrent_read(queries, keys_in, values_in, in_log, forget_log, state_matrix, state_norm, state_max):
    scaled_query = queries.astype(jnp.float32) * queries.shape[-1] ** (-0.5)
    key_float = keys_in.astype(jnp.float32)
    value_float = values_in.astype(jnp.float32)
    new_max = jnp.maximum(forget_log + state_max, in_log)
    carried = jnp.exp(forget_log + state_max - new_max)
    fresh_weight = jnp.exp(in_log - new_max)
    new_matrix = carried[..., None, None] * state_matrix + fresh_weight[..., None, None] * key_float[..., :, None] * value_float[..., None, :]
    new_norm = carried[..., None] * state_norm + fresh_weight[..., None] * key_float
    numerator = lax.optimization_barrier(jnp.sum(new_matrix * scaled_query[..., :, None], axis=-2))
    denominator = lax.optimization_barrier(jnp.sum(new_norm * scaled_query, axis=-1))
    floor_value = jnp.maximum(jnp.abs(denominator), jnp.exp(-new_max))
    readout = numerator / floor_value[..., None]
    return (readout, new_matrix, new_norm, new_max)

def head_output(readout, outgates, head_gain):
    scaled = readout * lax.rsqrt(lax.optimization_barrier(jnp.mean(readout * readout, axis=-1, keepdims=True)) + EPSILON)
    rows_count, heads_count, head_width = readout.shape
    gated_rows = scaled.reshape(rows_count, heads_count * head_width) * head_gain.astype(jnp.float32)[None, :]
    gated_rows = gated_rows * jax.nn.sigmoid(outgates.astype(jnp.float32))
    return gated_rows.astype(jnp.bfloat16)

def expert_slots(routes, groups, capacity, experts_all):
    row_total = routes.shape[0]
    chosen = (routes[:, :, None] == jnp.arange(experts_all, dtype=jnp.int32)[None, None, :]).astype(jnp.int32)
    per_row = lax.optimization_barrier(jnp.sum(chosen, axis=1))
    grouped = per_row.reshape(groups, row_total // groups, experts_all)
    earlier = (jnp.cumsum(grouped, axis=1) - grouped).reshape(row_total, experts_all)
    rank_in = lax.optimization_barrier(jnp.sum(chosen * earlier[:, None, :], axis=2))
    group_of = jnp.arange(row_total, dtype=jnp.int32) // (row_total // groups)
    return (routes * (groups * capacity) + group_of[:, None] * capacity + rank_in).astype(jnp.int32)

def reference(tokens, mix_gain, w_query, w_key, w_value, w_outgate, w_igate, w_fgate, igate_bias, fgate_bias, head_gain, w_mixout, state_matrix, state_norm, state_max, ffn_gain, dense_mix, w_dense_gate, w_dense_up, w_dense_down, routes, route_weights, w_exp_gate, w_exp_up, w_exp_down):
    token_float = tokens.astype(jnp.float32)
    inverse = lax.rsqrt(lax.optimization_barrier(jnp.mean(token_float * token_float, axis=1)) + EPSILON)
    normed = (token_float * inverse[:, None] * mix_gain.astype(jnp.float32)[None, :]).astype(jnp.bfloat16)
    queries = jnp.dot(normed, w_query, preferred_element_type=jnp.float32).astype(jnp.bfloat16).reshape(BATCH, H, DK)
    keys_in = jnp.dot(normed, w_key, preferred_element_type=jnp.float32).astype(jnp.bfloat16).reshape(BATCH, H, DK)
    values_in = jnp.dot(normed, w_value, preferred_element_type=jnp.float32).astype(jnp.bfloat16).reshape(BATCH, H, DV)
    outgates = jnp.dot(normed, w_outgate, preferred_element_type=jnp.float32).astype(jnp.bfloat16)
    in_pre = jnp.dot(normed, w_igate, preferred_element_type=jnp.float32)
    forget_pre = jnp.dot(normed, w_fgate, preferred_element_type=jnp.float32)
    in_log, forget_log = gate_logs(in_pre, forget_pre, igate_bias, fgate_bias)
    readout, new_matrix, new_norm, new_max = recurrent_read(queries, keys_in, values_in, in_log, forget_log, state_matrix, state_norm, state_max)
    heads_out = head_output(readout, outgates, head_gain)
    mixer = lax.optimization_barrier(jnp.dot(heads_out, w_mixout, preferred_element_type=jnp.float32).astype(jnp.bfloat16))
    hidden_state = lax.optimization_barrier((token_float + mixer.astype(jnp.float32)).astype(jnp.bfloat16))
    hidden_float = hidden_state.astype(jnp.float32)
    gain_float = ffn_gain.astype(jnp.float32)
    inverse_two = lax.rsqrt(lax.optimization_barrier(jnp.mean(hidden_float * hidden_float, axis=1)) + EPSILON)
    dense_gate = inverse_two * lax.optimization_barrier(jnp.sum(hidden_float * gain_float[None, :] * dense_mix.astype(jnp.float32)[None, :], axis=1))
    normed_two = (hidden_float * inverse_two[:, None] * gain_float[None, :]).astype(jnp.bfloat16)
    dense_hidden = (jax.nn.silu(jnp.dot(normed_two, w_dense_gate, preferred_element_type=jnp.float32)) * jnp.dot(normed_two, w_dense_up, preferred_element_type=jnp.float32)).astype(jnp.bfloat16)
    dense = jnp.dot(dense_hidden, w_dense_down, preferred_element_type=jnp.float32)
    flat_index = expert_slots(routes, N_EP, CAP, EXPERTS).reshape(-1)
    slot_count = N_EP * CAP
    send_rows = jnp.zeros((EXPERTS * slot_count, D), jnp.bfloat16).at[flat_index].set(jnp.repeat(normed_two, TOPK, axis=0)).reshape(EXPERTS, slot_count, D)

    def run_expert(operands):
        gate_matrix, up_matrix, down_matrix, arrived = operands
        gate_part = jnp.dot(arrived, gate_matrix, preferred_element_type=jnp.float32)
        up_part = jnp.dot(arrived, up_matrix, preferred_element_type=jnp.float32)
        expert_hidden = (jax.nn.silu(gate_part) * up_part).astype(jnp.bfloat16)
        summed = jnp.zeros((arrived.shape[0], D), jnp.float32)
        for group_index in range(N_TP):
            lower = group_index * UNIT_GROUP
            expert_part = jnp.dot(expert_hidden[:, lower:lower + UNIT_GROUP], down_matrix[lower:lower + UNIT_GROUP], preferred_element_type=jnp.float32).astype(jnp.bfloat16)
            summed = summed + lax.optimization_barrier(expert_part).astype(jnp.float32)
        return summed
    returned = lax.map(run_expert, (w_exp_gate, w_exp_up, w_exp_down, send_rows))
    picked = returned.reshape(EXPERTS * slot_count, D)[flat_index].reshape(BATCH, TOPK, D)
    routed = lax.optimization_barrier(jnp.sum(picked * route_weights[:, :, None], axis=1))
    layer_out = (hidden_float + routed + jax.nn.sigmoid(dense_gate)[:, None] * dense).astype(jnp.bfloat16)
    return (layer_out, new_matrix, new_norm, new_max)
```

```python
import functools

import jax
import jax.numpy as jnp
from jax import lax
from jax.experimental import pallas as pl
from jax.experimental.pallas import tpu as pltpu
from jax.sharding import PartitionSpec as P

EPSILON = 1e-06
SOFT_CAP = 15.0
MESH = pl.DeviceIdType.MESH
F32 = jnp.float32
BF16 = jnp.bfloat16


def each(count, body):
    if count <= 8:
        for i in range(count):
            body(i)
    else:

        @pl.loop(0, count)
        def _(i):
            body(i)


def dot(a, b):
    return jnp.dot(a, b, preferred_element_type=F32)


def pick_lane(x, lane):
    lanes = lax.broadcasted_iota(jnp.int32, x.shape, 1)
    return jnp.sum(jnp.where(lanes == lane, x, 0.0), axis=1, keepdims=True)


def layer_kernel(
    n,
    tn,
    d_model,
    tokens_in,
    mix_gain_in,
    w_query,
    w_key,
    w_value,
    w_outgate,
    w_igate_in,
    w_fgate_in,
    igate_bias_in,
    fgate_bias_in,
    head_gain_in,
    w_mixout,
    state_matrix,
    state_norm_in,
    state_max_in,
    ffn_gain_in,
    dense_mix_in,
    w_dense_gate,
    w_dense_up,
    w_dense_down,
    routes_in,
    route_weights_in,
    w_exp_gate,
    w_exp_up,
    w_exp_down,
    layer_out,
    new_matrix,
    new_norm,
    new_max,
    tokens,
    mix_gain_v,
    w_igate,
    w_fgate,
    igate_bias,
    fgate_bias,
    head_gain_v,
    state_norm,
    state_max,
    ffn_gain_v,
    dense_mix_v,
    routes,
    route_weights,
    norm_out,
    max_out,
    wq,
    wk,
    wv,
    wo,
    wm,
    sm,
    wdg,
    wdu,
    wdd,
    weg,
    weu,
    wed,
    proj_send,
    proj_recv,
    gate_send,
    gate_recv,
    num,
    heads_all,
    mix_send,
    mix_recv,
    hid_own,
    y_all,
    stat_send,
    stat_recv,
    stat_all,
    inv_two,
    dense_send,
    dense_recv,
    unit_all,
    exp_acc,
    near_recv,
    far_recv,
    res_recv,
    out_acc,
    fin_send,
    fin_recv,
    fin_all,
    norm_wide,
    square,
    input_sem,
    local_sem,
    down_sem,
    ep_send,
    ep_recv,
    tp_send,
    tp_recv,
    pair_send,
    pair_recv,
):
    me = lax.axis_index("ep")
    mt = lax.axis_index("tp")
    rows, feats = tokens_in.shape
    chunk = min(rows, 128)
    chunks = rows // chunk
    seqs = state_norm_in.shape[0]
    heads, dk, dv = sm.shape[1], sm.shape[2], sm.shape[3]
    hk, hv = heads * dk, heads * dv
    units = wdg.shape[1]
    quarter = rows // tn
    per_chunk = chunk // seqs

    def fetch(i, src, dst):
        copy = pltpu.make_async_copy(src, dst, local_sem.at[i])
        copy.start()
        return copy

    def fetch_input(i, src, dst):
        copy = pltpu.make_async_copy(src, dst, input_sem.at[i])
        copy.start()
        return copy

    first_inputs = [
        fetch_input(i, src, dst)
        for i, (src, dst) in enumerate(
            (
                (tokens_in, tokens),
                (mix_gain_in, mix_gain_v),
                (w_igate_in, w_igate),
                (w_fgate_in, w_fgate),
            )
        )
    ]
    in_q = fetch(0, w_query, wq)
    in_k = fetch(1, w_key, wk)
    in_v = fetch(2, w_value, wv)
    in_o = fetch(3, w_outgate, wo)
    in_s = fetch(4, state_matrix, sm)
    later_inputs = [
        fetch_input(4 + i, src, dst)
        for i, (src, dst) in enumerate(
            (
                (igate_bias_in, igate_bias),
                (fgate_bias_in, fgate_bias),
                (head_gain_in, head_gain_v),
                (state_norm_in, state_norm),
                (state_max_in, state_max),
                (ffn_gain_in, ffn_gain_v),
                (dense_mix_in, dense_mix_v),
                (routes_in, routes),
                (route_weights_in, route_weights),
            )
        )
    ]
    in_m = fetch(5, w_mixout, wm)
    in_dg = fetch(6, w_dense_gate, wdg)
    in_du = fetch(7, w_dense_up, wdu)
    in_dd = fetch(8, w_dense_down, wdd)
    in_eg = fetch(9, w_exp_gate.at[0], weg)
    in_eu = fetch(10, w_exp_up.at[0], weu)

    def down_copy(t):
        if w_exp_down.shape[2] == n * feats:
            src = w_exp_down.at[0, :, pl.ds(pl.multiple_of(t * feats, 128), feats)]
        else:
            src = w_exp_down.at[t]
        return pltpu.make_async_copy(src, wed.at[t], down_sem.at[t])

    each(n, lambda t: down_copy(t).start())

    def ep_copy(phase, k, src, dst):
        return pltpu.make_async_remote_copy(
            src_ref=src,
            dst_ref=dst,
            send_sem=ep_send.at[phase, k - 1],
            recv_sem=ep_recv.at[phase, k - 1],
            device_id={"ep": lax.rem(me + k, n)},
            device_id_type=MESH,
        )

    def tp_copy(phase, k, src, dst):
        return pltpu.make_async_remote_copy(
            src_ref=src,
            dst_ref=dst,
            send_sem=tp_send.at[phase, k - 1],
            recv_sem=tp_recv.at[phase, k - 1],
            device_id={"tp": lax.rem(mt + k, tn)},
            device_id_type=MESH,
        )

    def peers(body):
        each(n - 1, lambda i: body(i + 1))

    def tp_peers(body):
        each(tn - 1, lambda i: body(i + 1))

    barrier = pltpu.get_barrier_semaphore()
    peers(
        lambda k: pl.semaphore_signal(
            barrier, inc=1, device_id={"ep": lax.rem(me + k, n)}, device_id_type=MESH
        )
    )
    tp_peers(
        lambda k: pl.semaphore_signal(
            barrier, inc=1, device_id={"tp": lax.rem(mt + k, tn)}, device_id_type=MESH
        )
    )

    def row_slice(c):
        return pl.ds(pl.multiple_of(c * chunk, chunk), chunk)

    for copy in first_inputs:
        copy.wait()
    mix_gain = mix_gain_v[...].astype(F32).reshape(1, feats)
    gate_weights = jnp.concatenate(
        [w_igate[...].astype(F32), w_fgate[...].astype(F32), jnp.zeros((128 - 2 * heads, feats), F32)],
        axis=0,
    ).astype(BF16)
    in_q.wait()
    in_k.wait()
    in_v.wait()
    in_o.wait()

    def project(c):
        tok = tokens[row_slice(c), :].astype(F32)
        scaled = (tok * mix_gain).astype(BF16)
        squares = jnp.sum(tok * tok, axis=1, keepdims=True)
        blocks = pl.ds(c * per_chunk, per_chunk)
        lanes = lax.broadcasted_iota(jnp.int32, (chunk, 128), 1)
        gates = lax.dot_general(
            scaled, gate_weights, (((1,), (1,)), ((), ())), preferred_element_type=F32
        ) + jnp.where(lanes == 2 * heads, squares, 0.0)
        gate_send[blocks] = gates.reshape(per_chunk, seqs, 128)
        offset = 0
        for weight in (wq, wk, wv, wo):
            width = weight.shape[1]
            part = dot(scaled, weight[...]).reshape(per_chunk, seqs, width)
            proj_send[blocks, :, offset : offset + width] = part.astype(BF16)
            offset += width

    each(chunks, project)
    pl.semaphore_wait(barrier, n + tn - 2)

    def proj_copy(k):
        t = lax.rem(me + k, n)
        return ep_copy(0, k, proj_send.at[t], proj_recv.at[k - 1])

    def gate_copy(k):
        t = lax.rem(me + k, n)
        return ep_copy(1, k, gate_send.at[t], gate_recv.at[k - 1])

    peers(lambda k: (gate_copy(k).start(), proj_copy(k).start()))

    proj_acc = num
    gate_total = gate_send[me]
    proj_acc[...] = proj_send[me].astype(F32)
    if n <= 8:
        for k in range(1, n):
            gate_copy(k).wait_recv()
            gate_total = gate_total + gate_recv[k - 1]
    else:
        peers(lambda k: gate_copy(k).wait_recv())
        gate_total = lax.fori_loop(1, n, lambda k, acc: acc + gate_recv[k - 1], gate_total)

    def take_proj(k):
        proj_copy(k).wait_recv()
        proj_acc[...] += proj_recv[k - 1].astype(F32)

    for copy in later_inputs:
        copy.wait()
    bias_lane = lax.broadcasted_iota(jnp.int32, (1, 128), 1)
    in_bias = jnp.zeros((1, 128), F32)
    forget_bias = jnp.zeros((1, 128), F32)
    for h in range(heads):
        in_bias = jnp.where(bias_lane == h, igate_bias[h], in_bias)
        forget_bias = jnp.where(bias_lane == h, fgate_bias[h], forget_bias)
    head_gain = head_gain_v[...].astype(F32).reshape(1, hv)
    ffn_gain = ffn_gain_v[...].astype(F32).reshape(1, feats)
    dense_mix = dense_mix_v[...].astype(F32).reshape(1, feats)

    inverse = lax.rsqrt(pick_lane(gate_total, 2 * heads) / d_model + EPSILON)
    gate_total = gate_total * inverse
    in_log = SOFT_CAP * jnp.tanh((gate_total + in_bias) / SOFT_CAP)
    forget_pre = pltpu.roll(gate_total, 128 - heads, 1)
    capped = SOFT_CAP * jnp.tanh((forget_pre + forget_bias) / SOFT_CAP)
    forget_log = jnp.minimum(capped, 0.0) - jnp.log1p(jnp.exp(-jnp.abs(capped)))
    square[...] = jnp.zeros_like(square)
    square[0:heads, 0:seqs] = state_max[...]
    moved = forget_log + square[...].T[0:seqs, :]
    top = jnp.maximum(moved, in_log)
    carried = jnp.exp(moved - top)
    fresh = jnp.exp(in_log - top)
    floor = jnp.exp(-top)
    top_square = jnp.concatenate([top, jnp.zeros((128 - seqs, 128), F32)], axis=0).T
    max_out[...] = top_square[0:heads, 0:seqs]
    max_copy = pltpu.make_async_copy(max_out, new_max, input_sem.at[13])
    max_copy.start()
    head_lane = lax.broadcasted_iota(jnp.int32, (seqs, hk), 1) // dk
    carried_cols = [pick_lane(carried, h) for h in range(heads)]
    floor_cols = [pick_lane(floor, h) for h in range(heads)]
    carried_wide = jnp.zeros((seqs, hk), F32)
    fresh_wide = jnp.zeros((seqs, hk), F32)
    for h in range(heads):
        carried_wide = jnp.where(head_lane == h, carried_cols[h], carried_wide)
        fresh_wide = jnp.where(head_lane == h, pick_lane(fresh, h), fresh_wide)

    peers(take_proj)

    def rounded(lo, width):
        return (proj_acc[:, lo : lo + width] * inverse).astype(BF16).astype(F32)

    query = rounded(0, hk) * dk ** (-0.5)
    key = rounded(hk, hk) * fresh_wide
    value = rounded(2 * hk, hv)
    outgate = rounded(2 * hk + hv, hv)
    for h in range(heads):
        norm_wide[:, h * dk : (h + 1) * dk] = state_norm[:, h, :]
    norm = carried_wide * norm_wide[...] + key
    for h in range(heads):
        norm_out[:, h, :] = norm[:, h * dk : (h + 1) * dk]
    norm_copy = pltpu.make_async_copy(norm_out, new_norm, input_sem.at[14])
    norm_copy.start()
    product = norm * query
    padding = jnp.zeros((128 - seqs, hk), F32)
    query_t = jnp.concatenate([query, padding], axis=0).T
    key_t = jnp.concatenate([key, padding], axis=0).T
    in_s.wait()
    for h in range(heads):
        hs = slice(h * dk, (h + 1) * dk)
        readouts = []
        for r in range(seqs):
            state = (
                carried_cols[h][r : r + 1, :] * sm[r, h]
                + key_t[hs, r : r + 1] * value[r : r + 1, h * dv : (h + 1) * dv]
            )
            sm[r, h] = state
            readouts.append(jnp.sum(state * query_t[hs, r : r + 1], axis=0, keepdims=True))
        numerator = jnp.concatenate(readouts, axis=0)
        denominator = jnp.sum(jnp.where(head_lane == h, product, 0.0), axis=1, keepdims=True)
        readout = numerator / jnp.maximum(jnp.abs(denominator), floor_cols[h])
        cols = slice(h * dv, (h + 1) * dv)
        scale = lax.rsqrt(jnp.mean(readout * readout, axis=1, keepdims=True) + EPSILON)
        gated = readout * scale * head_gain[:, cols]
        gated = gated * jax.nn.sigmoid(outgate[:, cols])
        heads_all[me, :, cols] = gated.astype(BF16)

    def heads_copy(k):
        return ep_copy(2, k, heads_all.at[me], heads_all.at[me])

    peers(lambda k: heads_copy(k).start())
    state_out = pltpu.make_async_copy(sm, new_matrix, local_sem.at[11])
    state_out.start()

    in_m.wait()
    peers(lambda k: heads_copy(k).wait_recv())

    def mix_rows(c):
        held = heads_all[pl.ds(c * per_chunk, per_chunk)].reshape(chunk, hv)
        mix_send[row_slice(c), :] = dot(held, wm[...]).astype(BF16)

    each(chunks, mix_rows)

    def quarter_of(t):
        return pl.ds(pl.multiple_of(t * quarter, quarter), quarter)

    def mix_copy(k):
        return tp_copy(
            0, k, mix_send.at[quarter_of(lax.rem(mt + k, tn)), :], mix_recv.at[k - 1]
        )

    tp_peers(lambda k: mix_copy(k).start())
    mine = quarter_of(mt)
    near = mt + 1 - 2 * lax.rem(mt, 2)
    far = lax.rem(mt + 2, tn)
    both = lax.rem(near + 2, tn)
    mixed = mix_send[mine, :].astype(F32)
    for k in range(1, tn):
        mix_copy(k).wait_recv()
        mixed = mixed + mix_recv[k - 1].astype(F32)
    hidden = (tokens[mine, :].astype(F32) + mixed.astype(BF16).astype(F32)).astype(BF16)
    held = hidden.astype(F32)
    hid_own[...] = held
    gained = held * ffn_gain
    y_all[me, mine, :] = gained.astype(BF16)
    squares = jnp.sum(held * held, axis=1, keepdims=True)
    gate_dot = jnp.sum(gained * dense_mix, axis=1, keepdims=True)
    piece = min(quarter, 128)
    pieces = quarter // piece
    lanes = lax.broadcasted_iota(jnp.int32, (quarter, 128), 1)
    stats = jnp.where(lanes == 0, squares, jnp.where(lanes == 1, gate_dot, 0.0))
    for j in range(pieces):
        block = stats[j * piece : (j + 1) * piece, :]
        if piece < 128:
            block = jnp.concatenate([block, jnp.zeros((128 - piece, 128), F32)], axis=0)
        stat_send[j] = block.T[0:8, :]

    def part_copy(partner, sems, k, src, dst):
        return pltpu.make_async_remote_copy(
            src_ref=src,
            dst_ref=dst,
            send_sem=pair_send.at[sems, k],
            recv_sem=pair_recv.at[sems, k],
            device_id={"tp": partner},
            device_id_type=MESH,
        )

    def source_of(k):
        return lax.rem(me + n - k, n)

    def target_of(k):
        return lax.rem(me + k, n)

    def y_copy(k):
        return ep_copy(3, k, y_all.at[me, mine, :], y_all.at[me, mine, :])

    def spread(partner, sems, k, rows_at):
        view = y_all.at[source_of(k), quarter_of(rows_at), :]
        return part_copy(partner, sems, k, view, view)

    def y_far(k):
        return spread(far, 0, k, mt)

    def y_near(k):
        return spread(near, 1, k, mt)

    def y_near_far(k):
        return spread(near, 2, k, far)

    def stat_copy(k):
        return ep_copy(4, k, stat_send, stat_recv.at[k - 1])

    def stat_tp(k):
        return tp_copy(1, k, stat_all.at[mt], stat_all.at[mt])

    def dense_copy(k):
        return ep_copy(5, k, dense_send.at[target_of(k)], dense_recv.at[k - 1])

    y_far(0).start()
    peers(lambda k: (stat_copy(k).start(), y_copy(k).start()))
    y_near(0).start()
    y_far(0).wait_recv()
    y_near_far(0).start()
    in_dg.wait()
    in_du.wait()
    y_near(0).wait_recv()
    y_near_far(0).wait_recv()

    def dense_rows(c):
        held = y_all[me, row_slice(c), :]
        blocks = pl.ds(c * per_chunk, per_chunk)
        for lo, weight in ((0, wdg), (units, wdu)):
            part = dot(held, weight[...]).reshape(per_chunk, seqs, units)
            dense_send[blocks, :, lo : lo + units] = part.astype(BF16)

    each(chunks, dense_rows)
    peers(lambda k: dense_copy(k).start())

    if n <= 8:
        stat_total = stat_send[...]
        for k in range(1, n):
            stat_copy(k).wait_recv()
            stat_total = stat_total + stat_recv[k - 1]
    else:
        peers(lambda k: stat_copy(k).wait_recv())
        stat_total = lax.fori_loop(1, n, lambda k, acc: acc + stat_recv[k - 1], stat_send[...])
    stat_all[mt] = stat_total
    tp_peers(lambda k: stat_tp(k).start())

    in_eg.wait()
    in_eu.wait()

    def expert_block(source, first):
        feat_rows = pl.ds(pl.multiple_of(source * feats, feats), feats)

        def body(c):
            held = y_all[source, row_slice(c), :]
            for lo, weight in ((0, weg), (units, weu)):
                cols = slice(lo, lo + units)
                part = dot(held, weight[feat_rows, :])
                if first:
                    exp_acc[row_slice(c), cols] = part
                else:
                    exp_acc[row_slice(c), cols] += part

        each(chunks, body)

    def forward(k):
        y_copy(k).wait_recv()
        y_far(k).start()
        y_near(k).start()

    def forward_far(k):
        y_far(k).wait_recv()
        y_near_far(k).start()

    def expert_step(k):
        y_near(k).wait_recv()
        y_near_far(k).wait_recv()
        expert_block(source_of(k), False)

    def staged(stages, least):
        if n <= 8:
            for i in range(least, n + len(stages) - 1):
                for late, stage in enumerate(stages):
                    if least <= i - late < n:
                        stage(i - late)
        else:
            for stage in stages:
                each(n - least, lambda i, stage=stage: stage(i + least))

    expert_block(me, True)
    staged((forward, forward_far, expert_step), 1)

    tp_peers(lambda k: stat_tp(k).wait_recv())
    for q in range(tn):
        for j in range(pieces):
            total = stat_all[q, j]
            columns = jnp.concatenate([total, jnp.zeros((120, 128), F32)], axis=0).T
            scale = lax.rsqrt(pick_lane(columns, 0) / d_model + EPSILON)
            at = q * quarter + j * piece
            inv_two[at : at + piece, :] = jnp.broadcast_to(scale, (128, 128))[0:piece]

    dense_total = dense_send[me].astype(F32)
    if n <= 8:
        for k in range(1, n):
            dense_copy(k).wait_recv()
            dense_total = dense_total + dense_recv[k - 1].astype(F32)
    else:
        peers(lambda k: dense_copy(k).wait_recv())
        dense_total = lax.fori_loop(
            1, n, lambda k, acc: acc + dense_recv[k - 1].astype(F32), dense_total
        )
    seq_scale = inv_two[pl.ds(pl.multiple_of(me * seqs, seqs), seqs), 0:1]
    dense_total = dense_total * seq_scale
    unit_all[me] = (
        jax.nn.silu(dense_total[:, 0:units]) * dense_total[:, units : 2 * units]
    ).astype(BF16)

    def unit_copy(k):
        return ep_copy(6, k, unit_all.at[me], unit_all.at[me])

    peers(lambda k: unit_copy(k).start())

    def expert_units(c):
        picks = routes[:, row_slice(c)] == me
        weight = jnp.sum(
            jnp.where(picks, route_weights[:, row_slice(c)], 0.0), axis=0, keepdims=True
        )
        weight = pick_lane(jnp.broadcast_to(weight, (chunk, chunk)).T, 0)
        scale = inv_two[row_slice(c), 0:1]
        gate = exp_acc[row_slice(c), 0:units] * scale
        up = exp_acc[row_slice(c), units : 2 * units] * scale
        exp_acc[row_slice(c), 0:units] = jax.nn.silu(gate) * up * weight

    each(chunks, expert_units)
    peers(lambda k: y_copy(k).wait_send())
    each(n, lambda k: (y_far(k).wait_send(), y_near(k).wait_send()))
    each(n, lambda k: y_near_far(k).wait_send())

    def result_view(k, rows_at):
        return y_all.at[target_of(k), quarter_of(rows_at), :]

    def res_near(k):
        return part_copy(near, 3, k, result_view(k, near), near_recv.at[k, 0])

    def res_near_far(k):
        return part_copy(near, 4, k, result_view(k, both), near_recv.at[k, 1])

    def res_far(k):
        return part_copy(far, 5, k, result_view(k, far), far_recv.at[k])

    def res_copy(k):
        return ep_copy(7, k, result_view(k, mt), res_recv.at[k - 1])

    def result_step(k):
        t = target_of(k)
        down_copy(t).wait()

        def body(c):
            held = exp_acc[row_slice(c), 0:units].astype(BF16)
            y_all[t, row_slice(c), :] = dot(held, wed[t]).astype(BF16)

        each(chunks, body)
        res_near_far(k).start()
        res_near(k).start()

    def result_far(k):
        res_near_far(k).wait_recv()
        summed = y_all[target_of(k), quarter_of(far), :].astype(F32) + near_recv[k, 1].astype(F32)
        y_all[target_of(k), quarter_of(far), :] = summed.astype(BF16)
        res_far(k).start()

    def result_sum(k):
        res_near(k).wait_recv()
        res_far(k).wait_recv()
        return (
            y_all[target_of(k), mine, :].astype(F32)
            + near_recv[k, 0].astype(F32)
            + far_recv[k].astype(F32)
        )

    def result_out(k):
        y_all[target_of(k), mine, :] = result_sum(k).astype(BF16)
        res_copy(k).start()

    staged((result_step, result_far, result_out), 1)

    result_step(0)
    in_dd.wait()
    peers(lambda k: unit_copy(k).wait_recv())

    def down_rows(c):
        hidden_units = unit_all[pl.ds(c * per_chunk, per_chunk)].reshape(chunk, units)
        fin_send[row_slice(c), :] = dot(hidden_units, wdd[...]).astype(BF16)

    each(chunks, down_rows)

    def fin_copy(k):
        return tp_copy(
            2, k, fin_send.at[quarter_of(lax.rem(mt + k, tn)), :], fin_recv.at[k - 1]
        )

    tp_peers(lambda k: fin_copy(k).start())
    result_far(0)
    dense = fin_send[mine, :].astype(F32)
    for k in range(1, tn):
        fin_copy(k).wait_recv()
        dense = dense + fin_recv[k - 1].astype(F32)
    gates = []
    for j in range(pieces):
        columns = jnp.concatenate([stat_total[j], jnp.zeros((120, 128), F32)], axis=0).T
        scale = lax.rsqrt(pick_lane(columns, 0) / d_model + EPSILON)
        gates.append(jax.nn.sigmoid(scale * pick_lane(columns, 1))[0:piece])
    gate = gates[0] if pieces == 1 else jnp.concatenate(gates, axis=0)
    out_acc[...] = result_sum(0) + gate * dense

    def take_result(k):
        res_copy(k).wait_recv()
        out_acc[...] += res_recv[k - 1].astype(F32)

    peers(take_result)
    fin_all[mine, :] = (hid_own[...] + out_acc[...]).astype(BF16)

    def all_copy(k):
        return tp_copy(3, k, fin_all.at[mine, :], fin_all.at[mine, :])

    tp_peers(lambda k: all_copy(k).start())
    tp_peers(lambda k: all_copy(k).wait_recv())
    layer_copy = pltpu.make_async_copy(fin_all, layer_out, input_sem.at[15])
    layer_copy.start()
    max_copy.wait()
    norm_copy.wait()
    state_out.wait()
    for copies in (
        proj_copy,
        gate_copy,
        heads_copy,
        stat_copy,
        dense_copy,
        unit_copy,
        res_copy,
    ):
        peers(lambda k, copies=copies: copies(k).wait_send())
    for copies in (res_near, res_near_far, res_far):
        each(n, lambda k, copies=copies: copies(k).wait_send())
    for copies in (mix_copy, stat_tp, fin_copy, all_copy):
        tp_peers(lambda k, copies=copies: copies(k).wait_send())
    layer_copy.wait()


def finish_kernel(parts, layer_in, matrix_in, norm_in, max_in, layer_out, matrix_out, norm_out, max_out, layer_v, matrix_v, norm_v, max_v, in_sem, out_sem):
    seqs = matrix_in.shape[0] // parts
    pairs = [
        (matrix_in.at[pl.ds(i * seqs, seqs)], matrix_v.at[pl.ds(i * seqs, seqs)], matrix_out.at[pl.ds(i * seqs, seqs)])
        for i in range(parts)
    ] + [(layer_in, layer_v, layer_out), (norm_in, norm_v, norm_out), (max_in, max_v, max_out)]
    into = [pltpu.make_async_copy(src, held, in_sem.at[i]) for i, (src, held, _) in enumerate(pairs)]
    out = [pltpu.make_async_copy(held, dst, out_sem.at[i]) for i, (_, held, dst) in enumerate(pairs)]
    for copy in into:
        copy.start()
    for first, second in zip(into, out):
        first.wait()
        second.start()
    for copy in out:
        copy.wait()


def finish(layer_out, new_matrix, new_norm, new_max):
    parts = 8
    arrays = (layer_out, new_matrix, new_norm, new_max)
    hbm = pl.BlockSpec(memory_space=pl.ANY)
    return pl.pallas_call(
        functools.partial(finish_kernel, parts),
        out_shape=tuple(jax.ShapeDtypeStruct(a.shape, a.dtype) for a in arrays),
        in_specs=[hbm] * 4,
        out_specs=(hbm,) * 4,
        scratch_shapes=[pltpu.VMEM(a.shape, a.dtype) for a in arrays]
        + [pltpu.SemaphoreType.DMA((parts + 3,)), pltpu.SemaphoreType.DMA((parts + 3,))],
        compiler_params=pltpu.CompilerParams(vmem_limit_bytes=66_900_000),
    )(*arrays)

def on_device(
    n,
    tn,
    tokens,
    mix_gain,
    w_query,
    w_key,
    w_value,
    w_outgate,
    w_igate,
    w_fgate,
    igate_bias,
    fgate_bias,
    head_gain,
    w_mixout,
    state_matrix,
    state_norm,
    state_max,
    ffn_gain,
    dense_mix,
    w_dense_gate,
    w_dense_up,
    w_dense_down,
    routes,
    route_weights,
    w_exp_gate,
    w_exp_up,
    w_exp_down,
):
    rows, feats = tokens.shape
    seqs, heads, dk, dv = state_matrix.shape
    hk, hv = heads * dk, heads * dv
    units = w_dense_gate.shape[1]
    wide = 2 * hk + 2 * hv
    quarter = rows // tn
    pieces = max(1, quarter // 128)
    hbm = pl.BlockSpec(memory_space=pl.ANY)
    dma = pltpu.SemaphoreType.DMA
    scratch = [
        pltpu.VMEM(tokens.shape, BF16),
        pltpu.VMEM(mix_gain.shape, BF16),
        pltpu.VMEM((heads, feats), BF16),
        pltpu.VMEM((heads, feats), BF16),
        pltpu.SMEM(igate_bias.shape, F32),
        pltpu.SMEM(fgate_bias.shape, F32),
        pltpu.VMEM(head_gain.shape, BF16),
        pltpu.VMEM(state_norm.shape, F32),
        pltpu.VMEM((heads, seqs), F32),
        pltpu.VMEM(ffn_gain.shape, BF16),
        pltpu.VMEM(dense_mix.shape, BF16),
        pltpu.VMEM((routes.shape[1], rows), jnp.int32),
        pltpu.VMEM((routes.shape[1], rows), F32),
        pltpu.VMEM(state_norm.shape, F32),
        pltpu.VMEM((heads, seqs), F32),
        pltpu.VMEM(w_query.shape, BF16),
        pltpu.VMEM(w_key.shape, BF16),
        pltpu.VMEM(w_value.shape, BF16),
        pltpu.VMEM(w_outgate.shape, BF16),
        pltpu.VMEM(w_mixout.shape, BF16),
        pltpu.VMEM(state_matrix.shape, F32),
        pltpu.VMEM(w_dense_gate.shape, BF16),
        pltpu.VMEM(w_dense_up.shape, BF16),
        pltpu.VMEM(w_dense_down.shape, BF16),
        pltpu.VMEM(w_exp_gate.shape[1:], BF16),
        pltpu.VMEM(w_exp_up.shape[1:], BF16),
        pltpu.VMEM((n, units, feats), BF16),
        pltpu.VMEM((n, seqs, wide), BF16),
        pltpu.VMEM((n - 1, seqs, wide), BF16),
        pltpu.VMEM((n, seqs, 128), F32),
        pltpu.VMEM((n - 1, seqs, 128), F32),
        pltpu.VMEM((seqs, wide), F32),
        pltpu.VMEM((n, seqs, hv), BF16),
        pltpu.VMEM((rows, feats), BF16),
        pltpu.VMEM((tn - 1, quarter, feats), BF16),
        pltpu.VMEM((quarter, feats), F32),
        pltpu.VMEM((n, rows, feats), BF16),
        pltpu.VMEM((pieces, 8, 128), F32),
        pltpu.VMEM((n - 1, pieces, 8, 128), F32),
        pltpu.VMEM((tn, pieces, 8, 128), F32),
        pltpu.VMEM((rows, 128), F32),
        pltpu.VMEM((n, seqs, 2 * units), BF16),
        pltpu.VMEM((n - 1, seqs, 2 * units), BF16),
        pltpu.VMEM((n, seqs, units), BF16),
        pltpu.VMEM((rows, 2 * units), F32),
        pltpu.VMEM((n, 2, quarter, feats), BF16),
        pltpu.VMEM((n, quarter, feats), BF16),
        pltpu.VMEM((n - 1, quarter, feats), BF16),
        pltpu.VMEM((quarter, feats), F32),
        pltpu.VMEM((rows, feats), BF16),
        pltpu.VMEM((tn - 1, quarter, feats), BF16),
        pltpu.VMEM((rows, feats), BF16),
        pltpu.VMEM((seqs, hk), F32),
        pltpu.VMEM((128, 128), F32),
        dma((16,)),
        dma((12,)),
        dma((n,)),
        dma((8, n - 1)),
        dma((8, n - 1)),
        dma((4, tn - 1)),
        dma((4, tn - 1)),
        dma((6, n)),
        dma((6, n)),
    ]
    layer_out, new_matrix, new_norm, new_max = pl.pallas_call(
        functools.partial(layer_kernel, n, tn, n * feats),
        out_shape=(
            jax.ShapeDtypeStruct((rows, feats), BF16),
            jax.ShapeDtypeStruct(state_matrix.shape, F32),
            jax.ShapeDtypeStruct(state_norm.shape, F32),
            jax.ShapeDtypeStruct((heads, seqs), F32),
        ),
        in_specs=[hbm] * 25,
        out_specs=(hbm,) * 4,
        scratch_shapes=scratch,
        compiler_params=pltpu.CompilerParams(
            collective_id=0, has_side_effects=True, vmem_limit_bytes=66_900_000
        ),
    )(
        tokens,
        mix_gain,
        w_query,
        w_key,
        w_value,
        w_outgate,
        w_igate.T,
        w_fgate.T,
        igate_bias,
        fgate_bias,
        head_gain,
        w_mixout,
        state_matrix,
        state_norm,
        state_max.T,
        ffn_gain,
        dense_mix,
        w_dense_gate,
        w_dense_up,
        w_dense_down,
        routes.T,
        route_weights.T,
        w_exp_gate,
        w_exp_up,
        w_exp_down,
    )
    layer_out, new_matrix, new_norm, new_max = finish(layer_out, new_matrix, new_norm, new_max)
    return layer_out, new_matrix, new_norm, new_max.T


def wide_kernel(
    n,
    tn,
    d_model,
    tokens,
    small,
    w_gates,
    state_norm,
    state_max,
    routes,
    route_weights,
    w_query,
    w_key,
    w_value,
    w_outgate,
    w_mixout,
    state_matrix,
    w_dense_gate,
    w_dense_up,
    w_dense_down,
    w_exp_gate,
    w_exp_up,
    w_exp_down,
    layer_out,
    new_matrix,
    new_norm,
    new_max,
    wq,
    wk,
    wv,
    wo,
    wm,
    sm,
    wdg,
    wdu,
    wdd,
    weg,
    weu,
    wed,
    proj_send,
    proj_recv,
    gate_send,
    gate_recv,
    num,
    heads_all,
    mix_send,
    mix_recv,
    hid_own,
    y_all,
    stat_send,
    stat_recv,
    stat_all,
    inv_two,
    dense_send,
    dense_recv,
    unit_all,
    exp_acc,
    near_recv,
    far_recv,
    res_recv,
    out_acc,
    fin_send,
    fin_recv,
    fin_all,
    norm_wide,
    square,
    local_sem,
    down_sem,
    ep_send,
    ep_recv,
    tp_send,
    tp_recv,
    pair_send,
    pair_recv,
):
    me = lax.axis_index("ep")
    mt = lax.axis_index("tp")
    rows, feats = tokens.shape
    chunk = min(rows, 128)
    chunks = rows // chunk
    seqs = state_norm.shape[0]
    heads, dk, dv = sm.shape[1], sm.shape[2], sm.shape[3]
    hk, hv = heads * dk, heads * dv
    units = wdg.shape[1]
    quarter = rows // tn
    per_chunk = chunk // seqs

    def fetch(i, src, dst):
        copy = pltpu.make_async_copy(src, dst, local_sem.at[i])
        copy.start()
        return copy

    in_q = fetch(0, w_query, wq)
    in_k = fetch(1, w_key, wk)
    in_v = fetch(2, w_value, wv)
    in_o = fetch(3, w_outgate, wo)
    in_s = fetch(4, state_matrix, sm)
    in_m = fetch(5, w_mixout, wm)
    in_dg = fetch(6, w_dense_gate, wdg)
    in_du = fetch(7, w_dense_up, wdu)
    in_dd = fetch(8, w_dense_down, wdd)
    in_eg = fetch(9, w_exp_gate.at[0], weg)
    in_eu = fetch(10, w_exp_up.at[0], weu)

    def down_copy(t):
        if w_exp_down.shape[2] == n * feats:
            src = w_exp_down.at[0, :, pl.ds(pl.multiple_of(t * feats, 128), feats)]
        else:
            src = w_exp_down.at[t]
        return pltpu.make_async_copy(src, wed.at[t], down_sem.at[t])

    each(n, lambda t: down_copy(t).start())

    def ep_copy(phase, k, src, dst):
        return pltpu.make_async_remote_copy(
            src_ref=src,
            dst_ref=dst,
            send_sem=ep_send.at[phase, k - 1],
            recv_sem=ep_recv.at[phase, k - 1],
            device_id={"ep": lax.rem(me + k, n)},
            device_id_type=MESH,
        )

    def tp_copy(phase, k, src, dst):
        return pltpu.make_async_remote_copy(
            src_ref=src,
            dst_ref=dst,
            send_sem=tp_send.at[phase, k - 1],
            recv_sem=tp_recv.at[phase, k - 1],
            device_id={"tp": lax.rem(mt + k, tn)},
            device_id_type=MESH,
        )

    def peers(body):
        each(n - 1, lambda i: body(i + 1))

    def tp_peers(body):
        each(tn - 1, lambda i: body(i + 1))

    barrier = pltpu.get_barrier_semaphore()
    peers(
        lambda k: pl.semaphore_signal(
            barrier, inc=1, device_id={"ep": lax.rem(me + k, n)}, device_id_type=MESH
        )
    )
    tp_peers(
        lambda k: pl.semaphore_signal(
            barrier, inc=1, device_id={"tp": lax.rem(mt + k, tn)}, device_id_type=MESH
        )
    )

    def row_slice(c):
        return pl.ds(pl.multiple_of(c * chunk, chunk), chunk)

    in_q.wait()
    in_k.wait()
    in_v.wait()
    in_o.wait()

    def project(c):
        tok = tokens[row_slice(c), :].astype(F32)
        scaled = (tok * small[0:1, 0:feats]).astype(BF16)
        squares = jnp.sum(tok * tok, axis=1, keepdims=True)
        blocks = pl.ds(c * per_chunk, per_chunk)
        lanes = lax.broadcasted_iota(jnp.int32, (chunk, 128), 1)
        gates = lax.dot_general(
            scaled, w_gates[...], (((1,), (1,)), ((), ())), preferred_element_type=F32
        ) + jnp.where(lanes == 2 * heads, squares, 0.0)
        gate_send[blocks] = gates.reshape(per_chunk, seqs, 128)
        offset = 0
        for weight in (wq, wk, wv, wo):
            width = weight.shape[1]
            part = dot(scaled, weight[...]).reshape(per_chunk, seqs, width)
            proj_send[blocks, :, offset : offset + width] = part.astype(BF16)
            offset += width

    each(chunks, project)
    pl.semaphore_wait(barrier, n + tn - 2)

    def proj_copy(k):
        t = lax.rem(me + k, n)
        return ep_copy(0, k, proj_send.at[t], proj_recv.at[k - 1])

    def gate_copy(k):
        t = lax.rem(me + k, n)
        return ep_copy(1, k, gate_send.at[t], gate_recv.at[k - 1])

    peers(lambda k: (gate_copy(k).start(), proj_copy(k).start()))

    proj_acc = num
    gate_total = gate_send[me]
    proj_acc[...] = proj_send[me].astype(F32)
    if n <= 8:
        for k in range(1, n):
            gate_copy(k).wait_recv()
            gate_total = gate_total + gate_recv[k - 1]
    else:
        peers(lambda k: gate_copy(k).wait_recv())
        gate_total = lax.fori_loop(1, n, lambda k, acc: acc + gate_recv[k - 1], gate_total)

    def take_proj(k):
        proj_copy(k).wait_recv()
        proj_acc[...] += proj_recv[k - 1].astype(F32)

    inverse = lax.rsqrt(pick_lane(gate_total, 2 * heads) / d_model + EPSILON)
    gate_total = gate_total * inverse
    in_log = SOFT_CAP * jnp.tanh((gate_total + small[4:5, 0:128]) / SOFT_CAP)
    forget_pre = pltpu.roll(gate_total, 128 - heads, 1)
    capped = SOFT_CAP * jnp.tanh((forget_pre + small[5:6, 0:128]) / SOFT_CAP)
    forget_log = jnp.minimum(capped, 0.0) - jnp.log1p(jnp.exp(-jnp.abs(capped)))
    square[...] = jnp.zeros_like(square)
    square[0:heads, 0:seqs] = state_max[...]
    moved = forget_log + square[...].T[0:seqs, :]
    top = jnp.maximum(moved, in_log)
    carried = jnp.exp(moved - top)
    fresh = jnp.exp(in_log - top)
    floor = jnp.exp(-top)
    top_square = jnp.concatenate([top, jnp.zeros((128 - seqs, 128), F32)], axis=0).T
    new_max[...] = top_square[0:heads, 0:seqs]
    head_lane = lax.broadcasted_iota(jnp.int32, (seqs, hk), 1) // dk
    carried_cols = [pick_lane(carried, h) for h in range(heads)]
    floor_cols = [pick_lane(floor, h) for h in range(heads)]
    carried_wide = jnp.zeros((seqs, hk), F32)
    fresh_wide = jnp.zeros((seqs, hk), F32)
    for h in range(heads):
        carried_wide = jnp.where(head_lane == h, carried_cols[h], carried_wide)
        fresh_wide = jnp.where(head_lane == h, pick_lane(fresh, h), fresh_wide)

    peers(take_proj)

    def rounded(lo, width):
        return (proj_acc[:, lo : lo + width] * inverse).astype(BF16).astype(F32)

    query = rounded(0, hk) * dk ** (-0.5)
    key = rounded(hk, hk) * fresh_wide
    value = rounded(2 * hk, hv)
    outgate = rounded(2 * hk + hv, hv)
    for h in range(heads):
        norm_wide[:, h * dk : (h + 1) * dk] = state_norm[:, h, :]
    norm = carried_wide * norm_wide[...] + key
    new_norm[...] = norm
    product = norm * query
    padding = jnp.zeros((128 - seqs, hk), F32)
    query_t = jnp.concatenate([query, padding], axis=0).T
    key_t = jnp.concatenate([key, padding], axis=0).T
    in_s.wait()
    for h in range(heads):
        hs = slice(h * dk, (h + 1) * dk)
        readouts = []
        for r in range(seqs):
            state = (
                carried_cols[h][r : r + 1, :] * sm[r, h]
                + key_t[hs, r : r + 1] * value[r : r + 1, h * dv : (h + 1) * dv]
            )
            sm[r, h] = state
            readouts.append(jnp.sum(state * query_t[hs, r : r + 1], axis=0, keepdims=True))
        numerator = jnp.concatenate(readouts, axis=0)
        denominator = jnp.sum(jnp.where(head_lane == h, product, 0.0), axis=1, keepdims=True)
        readout = numerator / jnp.maximum(jnp.abs(denominator), floor_cols[h])
        cols = slice(h * dv, (h + 1) * dv)
        scale = lax.rsqrt(jnp.mean(readout * readout, axis=1, keepdims=True) + EPSILON)
        gated = readout * scale * small[3:4, cols]
        gated = gated * jax.nn.sigmoid(outgate[:, cols])
        heads_all[me, :, cols] = gated.astype(BF16)

    def heads_copy(k):
        return ep_copy(2, k, heads_all.at[me], heads_all.at[me])

    peers(lambda k: heads_copy(k).start())
    state_out = pltpu.make_async_copy(sm, new_matrix, local_sem.at[11])
    state_out.start()

    in_m.wait()
    peers(lambda k: heads_copy(k).wait_recv())

    def mix_rows(c):
        held = heads_all[pl.ds(c * per_chunk, per_chunk)].reshape(chunk, hv)
        mix_send[row_slice(c), :] = dot(held, wm[...]).astype(BF16)

    each(chunks, mix_rows)

    def quarter_of(t):
        return pl.ds(pl.multiple_of(t * quarter, quarter), quarter)

    def mix_copy(k):
        return tp_copy(
            0, k, mix_send.at[quarter_of(lax.rem(mt + k, tn)), :], mix_recv.at[k - 1]
        )

    tp_peers(lambda k: mix_copy(k).start())
    mine = quarter_of(mt)
    near = mt + 1 - 2 * lax.rem(mt, 2)
    far = lax.rem(mt + 2, tn)
    both = lax.rem(near + 2, tn)
    mixed = mix_send[mine, :].astype(F32)
    for k in range(1, tn):
        mix_copy(k).wait_recv()
        mixed = mixed + mix_recv[k - 1].astype(F32)
    hidden = (tokens[mine, :].astype(F32) + mixed.astype(BF16).astype(F32)).astype(BF16)
    held = hidden.astype(F32)
    hid_own[...] = held
    gained = held * small[1:2, 0:feats]
    y_all[me, mine, :] = gained.astype(BF16)
    squares = jnp.sum(held * held, axis=1, keepdims=True)
    gate_dot = jnp.sum(gained * small[2:3, 0:feats], axis=1, keepdims=True)
    piece = min(quarter, 128)
    pieces = quarter // piece
    lanes = lax.broadcasted_iota(jnp.int32, (quarter, 128), 1)
    stats = jnp.where(lanes == 0, squares, jnp.where(lanes == 1, gate_dot, 0.0))
    for j in range(pieces):
        block = stats[j * piece : (j + 1) * piece, :]
        if piece < 128:
            block = jnp.concatenate([block, jnp.zeros((128 - piece, 128), F32)], axis=0)
        stat_send[j] = block.T[0:8, :]

    def part_copy(partner, sems, k, src, dst):
        return pltpu.make_async_remote_copy(
            src_ref=src,
            dst_ref=dst,
            send_sem=pair_send.at[sems, k],
            recv_sem=pair_recv.at[sems, k],
            device_id={"tp": partner},
            device_id_type=MESH,
        )

    def source_of(k):
        return lax.rem(me + n - k, n)

    def target_of(k):
        return lax.rem(me + k, n)

    def y_copy(k):
        return ep_copy(3, k, y_all.at[me, mine, :], y_all.at[me, mine, :])

    def spread(partner, sems, k, rows_at):
        view = y_all.at[source_of(k), quarter_of(rows_at), :]
        return part_copy(partner, sems, k, view, view)

    def y_far(k):
        return spread(far, 0, k, mt)

    def y_near(k):
        return spread(near, 1, k, mt)

    def y_near_far(k):
        return spread(near, 2, k, far)

    def stat_copy(k):
        return ep_copy(4, k, stat_send, stat_recv.at[k - 1])

    def stat_tp(k):
        return tp_copy(1, k, stat_all.at[mt], stat_all.at[mt])

    def dense_copy(k):
        return ep_copy(5, k, dense_send.at[target_of(k)], dense_recv.at[k - 1])

    y_far(0).start()
    peers(lambda k: (stat_copy(k).start(), y_copy(k).start()))
    y_near(0).start()
    y_far(0).wait_recv()
    y_near_far(0).start()
    in_dg.wait()
    in_du.wait()
    y_near(0).wait_recv()
    y_near_far(0).wait_recv()

    def dense_rows(c):
        held = y_all[me, row_slice(c), :]
        blocks = pl.ds(c * per_chunk, per_chunk)
        for lo, weight in ((0, wdg), (units, wdu)):
            part = dot(held, weight[...]).reshape(per_chunk, seqs, units)
            dense_send[blocks, :, lo : lo + units] = part.astype(BF16)

    each(chunks, dense_rows)
    peers(lambda k: dense_copy(k).start())

    if n <= 8:
        stat_total = stat_send[...]
        for k in range(1, n):
            stat_copy(k).wait_recv()
            stat_total = stat_total + stat_recv[k - 1]
    else:
        peers(lambda k: stat_copy(k).wait_recv())
        stat_total = lax.fori_loop(1, n, lambda k, acc: acc + stat_recv[k - 1], stat_send[...])
    stat_all[mt] = stat_total
    tp_peers(lambda k: stat_tp(k).start())

    in_eg.wait()
    in_eu.wait()

    def expert_block(source, first):
        feat_rows = pl.ds(pl.multiple_of(source * feats, feats), feats)

        def body(c):
            held = y_all[source, row_slice(c), :]
            for lo, weight in ((0, weg), (units, weu)):
                cols = slice(lo, lo + units)
                part = dot(held, weight[feat_rows, :])
                if first:
                    exp_acc[row_slice(c), cols] = part
                else:
                    exp_acc[row_slice(c), cols] += part

        each(chunks, body)

    def forward(k):
        y_copy(k).wait_recv()
        y_far(k).start()
        y_near(k).start()

    def forward_far(k):
        y_far(k).wait_recv()
        y_near_far(k).start()

    def expert_step(k):
        y_near(k).wait_recv()
        y_near_far(k).wait_recv()
        expert_block(source_of(k), False)

    def staged(stages, least):
        if n <= 8:
            for i in range(least, n + len(stages) - 1):
                for late, stage in enumerate(stages):
                    if least <= i - late < n:
                        stage(i - late)
        else:
            for stage in stages:
                each(n - least, lambda i, stage=stage: stage(i + least))

    expert_block(me, True)
    staged((forward, forward_far, expert_step), 1)

    tp_peers(lambda k: stat_tp(k).wait_recv())
    for q in range(tn):
        for j in range(pieces):
            total = stat_all[q, j]
            columns = jnp.concatenate([total, jnp.zeros((120, 128), F32)], axis=0).T
            scale = lax.rsqrt(pick_lane(columns, 0) / d_model + EPSILON)
            at = q * quarter + j * piece
            inv_two[at : at + piece, :] = jnp.broadcast_to(scale, (128, 128))[0:piece]

    dense_total = dense_send[me].astype(F32)
    if n <= 8:
        for k in range(1, n):
            dense_copy(k).wait_recv()
            dense_total = dense_total + dense_recv[k - 1].astype(F32)
    else:
        peers(lambda k: dense_copy(k).wait_recv())
        dense_total = lax.fori_loop(
            1, n, lambda k, acc: acc + dense_recv[k - 1].astype(F32), dense_total
        )
    seq_scale = inv_two[pl.ds(pl.multiple_of(me * seqs, seqs), seqs), 0:1]
    dense_total = dense_total * seq_scale
    unit_all[me] = (
        jax.nn.silu(dense_total[:, 0:units]) * dense_total[:, units : 2 * units]
    ).astype(BF16)

    def unit_copy(k):
        return ep_copy(6, k, unit_all.at[me], unit_all.at[me])

    peers(lambda k: unit_copy(k).start())

    def expert_units(c):
        picks = routes[:, row_slice(c)] == me
        weight = jnp.sum(
            jnp.where(picks, route_weights[:, row_slice(c)], 0.0), axis=0, keepdims=True
        )
        weight = pick_lane(jnp.broadcast_to(weight, (chunk, chunk)).T, 0)
        scale = inv_two[row_slice(c), 0:1]
        gate = exp_acc[row_slice(c), 0:units] * scale
        up = exp_acc[row_slice(c), units : 2 * units] * scale
        exp_acc[row_slice(c), 0:units] = jax.nn.silu(gate) * up * weight

    each(chunks, expert_units)
    peers(lambda k: y_copy(k).wait_send())
    each(n, lambda k: (y_far(k).wait_send(), y_near(k).wait_send()))
    each(n, lambda k: y_near_far(k).wait_send())

    def result_view(k, rows_at):
        return y_all.at[target_of(k), quarter_of(rows_at), :]

    def res_near(k):
        return part_copy(near, 3, k, result_view(k, near), near_recv.at[k, 0])

    def res_near_far(k):
        return part_copy(near, 4, k, result_view(k, both), near_recv.at[k, 1])

    def res_far(k):
        return part_copy(far, 5, k, result_view(k, far), far_recv.at[k])

    def res_copy(k):
        return ep_copy(7, k, result_view(k, mt), res_recv.at[k - 1])

    def result_step(k):
        t = target_of(k)
        down_copy(t).wait()

        def body(c):
            held = exp_acc[row_slice(c), 0:units].astype(BF16)
            y_all[t, row_slice(c), :] = dot(held, wed[t]).astype(BF16)

        each(chunks, body)
        res_near_far(k).start()
        res_near(k).start()

    def result_far(k):
        res_near_far(k).wait_recv()
        summed = y_all[target_of(k), quarter_of(far), :].astype(F32) + near_recv[k, 1].astype(F32)
        y_all[target_of(k), quarter_of(far), :] = summed.astype(BF16)
        res_far(k).start()

    def result_sum(k):
        res_near(k).wait_recv()
        res_far(k).wait_recv()
        return (
            y_all[target_of(k), mine, :].astype(F32)
            + near_recv[k, 0].astype(F32)
            + far_recv[k].astype(F32)
        )

    def result_out(k):
        y_all[target_of(k), mine, :] = result_sum(k).astype(BF16)
        res_copy(k).start()

    staged((result_step, result_far, result_out), 1)

    result_step(0)
    in_dd.wait()
    peers(lambda k: unit_copy(k).wait_recv())

    def down_rows(c):
        hidden_units = unit_all[pl.ds(c * per_chunk, per_chunk)].reshape(chunk, units)
        fin_send[row_slice(c), :] = dot(hidden_units, wdd[...]).astype(BF16)

    each(chunks, down_rows)

    def fin_copy(k):
        return tp_copy(
            2, k, fin_send.at[quarter_of(lax.rem(mt + k, tn)), :], fin_recv.at[k - 1]
        )

    tp_peers(lambda k: fin_copy(k).start())
    result_far(0)
    dense = fin_send[mine, :].astype(F32)
    for k in range(1, tn):
        fin_copy(k).wait_recv()
        dense = dense + fin_recv[k - 1].astype(F32)
    gates = []
    for j in range(pieces):
        columns = jnp.concatenate([stat_total[j], jnp.zeros((120, 128), F32)], axis=0).T
        scale = lax.rsqrt(pick_lane(columns, 0) / d_model + EPSILON)
        gates.append(jax.nn.sigmoid(scale * pick_lane(columns, 1))[0:piece])
    gate = gates[0] if pieces == 1 else jnp.concatenate(gates, axis=0)
    out_acc[...] = result_sum(0) + gate * dense

    def take_result(k):
        res_copy(k).wait_recv()
        out_acc[...] += res_recv[k - 1].astype(F32)

    peers(take_result)
    fin_all[mine, :] = (hid_own[...] + out_acc[...]).astype(BF16)

    def all_copy(k):
        return tp_copy(3, k, fin_all.at[mine, :], fin_all.at[mine, :])

    tp_peers(lambda k: all_copy(k).start())
    tp_peers(lambda k: all_copy(k).wait_recv())
    layer_out[...] = fin_all[...]
    state_out.wait()
    for copies in (
        proj_copy,
        gate_copy,
        heads_copy,
        stat_copy,
        dense_copy,
        unit_copy,
        res_copy,
    ):
        peers(lambda k, copies=copies: copies(k).wait_send())
    for copies in (res_near, res_near_far, res_far):
        each(n, lambda k, copies=copies: copies(k).wait_send())
    for copies in (mix_copy, stat_tp, fin_copy, all_copy):
        tp_peers(lambda k, copies=copies: copies(k).wait_send())


def wide_on_device(
    n,
    tn,
    tokens,
    mix_gain,
    w_query,
    w_key,
    w_value,
    w_outgate,
    w_igate,
    w_fgate,
    igate_bias,
    fgate_bias,
    head_gain,
    w_mixout,
    state_matrix,
    state_norm,
    state_max,
    ffn_gain,
    dense_mix,
    w_dense_gate,
    w_dense_up,
    w_dense_down,
    routes,
    route_weights,
    w_exp_gate,
    w_exp_up,
    w_exp_down,
):
    rows, feats = tokens.shape
    seqs, heads, dk, dv = state_matrix.shape
    hk, hv = heads * dk, heads * dv
    units = w_dense_gate.shape[1]
    wide = 2 * hk + 2 * hv
    quarter = rows // tn
    pieces = max(1, quarter // 128)
    w_gates = jnp.pad(
        jnp.concatenate([w_igate.T, w_fgate.T], axis=0), ((0, 128 - 2 * heads), (0, 0))
    )
    width = max(feats, hv, 128)
    row_at = lax.broadcasted_iota(jnp.int32, (8, width), 0)
    small = jnp.zeros((8, width), F32)
    for at, row in enumerate(
        (mix_gain, ffn_gain, dense_mix, head_gain, igate_bias, fgate_bias)
    ):
        wide_row = jnp.pad(row.astype(F32), (0, width - row.shape[0]))
        small = jnp.where(row_at == at, wide_row[None, :], small)
    down = w_exp_down
    if feats % 128:
        down = w_exp_down[0].reshape(units, n, feats).transpose(1, 0, 2)
    vmem = pl.BlockSpec(memory_space=pltpu.VMEM)
    hbm = pl.BlockSpec(memory_space=pl.ANY)
    dma = pltpu.SemaphoreType.DMA
    scratch = [
        pltpu.VMEM(w_query.shape, BF16),
        pltpu.VMEM(w_key.shape, BF16),
        pltpu.VMEM(w_value.shape, BF16),
        pltpu.VMEM(w_outgate.shape, BF16),
        pltpu.VMEM(w_mixout.shape, BF16),
        pltpu.VMEM(state_matrix.shape, F32),
        pltpu.VMEM(w_dense_gate.shape, BF16),
        pltpu.VMEM(w_dense_up.shape, BF16),
        pltpu.VMEM(w_dense_down.shape, BF16),
        pltpu.VMEM(w_exp_gate.shape[1:], BF16),
        pltpu.VMEM(w_exp_up.shape[1:], BF16),
        pltpu.VMEM((n, units, feats), BF16),
        pltpu.VMEM((n, seqs, wide), BF16),
        pltpu.VMEM((n - 1, seqs, wide), BF16),
        pltpu.VMEM((n, seqs, 128), F32),
        pltpu.VMEM((n - 1, seqs, 128), F32),
        pltpu.VMEM((seqs, wide), F32),
        pltpu.VMEM((n, seqs, hv), BF16),
        pltpu.VMEM((rows, feats), BF16),
        pltpu.VMEM((tn - 1, quarter, feats), BF16),
        pltpu.VMEM((quarter, feats), F32),
        pltpu.VMEM((n, rows, feats), BF16),
        pltpu.VMEM((pieces, 8, 128), F32),
        pltpu.VMEM((n - 1, pieces, 8, 128), F32),
        pltpu.VMEM((tn, pieces, 8, 128), F32),
        pltpu.VMEM((rows, 128), F32),
        pltpu.VMEM((n, seqs, 2 * units), BF16),
        pltpu.VMEM((n - 1, seqs, 2 * units), BF16),
        pltpu.VMEM((n, seqs, units), BF16),
        pltpu.VMEM((rows, 2 * units), F32),
        pltpu.VMEM((n, 2, quarter, feats), BF16),
        pltpu.VMEM((n, quarter, feats), BF16),
        pltpu.VMEM((n - 1, quarter, feats), BF16),
        pltpu.VMEM((quarter, feats), F32),
        pltpu.VMEM((rows, feats), BF16),
        pltpu.VMEM((tn - 1, quarter, feats), BF16),
        pltpu.VMEM((rows, feats), BF16),
        pltpu.VMEM((seqs, hk), F32),
        pltpu.VMEM((128, 128), F32),
        dma((12,)),
        dma((n,)),
        dma((8, n - 1)),
        dma((8, n - 1)),
        dma((4, tn - 1)),
        dma((4, tn - 1)),
        dma((6, n)),
        dma((6, n)),
    ]
    layer_out, new_matrix, new_norm, new_max = pl.pallas_call(
        functools.partial(wide_kernel, n, tn, n * feats),
        out_shape=(
            jax.ShapeDtypeStruct((rows, feats), BF16),
            jax.ShapeDtypeStruct(state_matrix.shape, F32),
            jax.ShapeDtypeStruct((seqs, hk), F32),
            jax.ShapeDtypeStruct((heads, seqs), F32),
        ),
        in_specs=[vmem] * 7 + [hbm] * 12,
        out_specs=(vmem, hbm, vmem, vmem),
        scratch_shapes=scratch,
        compiler_params=pltpu.CompilerParams(
            collective_id=0, has_side_effects=True, vmem_limit_bytes=66_900_000
        ),
    )(
        tokens,
        small,
        w_gates,
        state_norm,
        state_max.T,
        routes.T,
        route_weights.T,
        w_query,
        w_key,
        w_value,
        w_outgate,
        w_mixout,
        state_matrix,
        w_dense_gate,
        w_dense_up,
        w_dense_down,
        w_exp_gate,
        w_exp_up,
        down,
    )
    return (
        layer_out,
        new_matrix,
        new_norm.reshape(seqs, heads, dk),
        new_max.T,
    )


def either(n, tn, tokens, *rest):
    part = on_device if tokens.shape[1] % 128 == 0 else wide_on_device
    return part(n, tn, tokens, *rest)


def solution(mesh):
    return jax.shard_map(
        functools.partial(either, mesh.shape["ep"], mesh.shape["tp"]),
        mesh=mesh,
        in_specs=(
            P(None, "ep"),
            P("ep"),
            P("ep", "tp"),
            P("ep", "tp"),
            P("ep", "tp"),
            P("ep", "tp"),
            P("ep", "tp"),
            P("ep", "tp"),
            P("tp"),
            P("tp"),
            P("tp"),
            P("tp", "ep"),
            P("ep", "tp", None, None),
            P("ep", "tp", None),
            P("ep", "tp"),
            P("ep"),
            P("ep"),
            P("ep", "tp"),
            P("ep", "tp"),
            P("tp", "ep"),
            P(),
            P(),
            P("ep", None, "tp"),
            P("ep", None, "tp"),
            P("ep", "tp", None),
        ),
        out_specs=(P(None, "ep"), P("ep", "tp", None, None), P("ep", "tp", None), P("ep", "tp")),
        check_vma=False,
    )
```

```python
import functools

import jax
import jax.numpy as jnp
from jax import lax
from jax.experimental import pallas as pl
from jax.experimental.pallas import tpu as pltpu
from jax.sharding import PartitionSpec as P

EPSILON = 1e-06
SOFT_CAP = 15.0
MESH = pl.DeviceIdType.MESH
F32 = jnp.float32
BF16 = jnp.bfloat16


def each(count, body):
    if count <= 8:
        for i in range(count):
            body(i)
    else:

        @pl.loop(0, count)
        def _(i):
            body(i)


def dot(a, b):
    return jnp.dot(a, b, preferred_element_type=F32)


def pick_lane(x, lane):
    lanes = lax.broadcasted_iota(jnp.int32, x.shape, 1)
    return jnp.sum(jnp.where(lanes == lane, x, 0.0), axis=1, keepdims=True)


def flip(index, mask):
    bit = 1
    while bit <= mask:
        if mask & bit:
            index = index + bit - 2 * bit * (index // bit % 2)
        bit *= 2
    return index


def layer_kernel(
    n,
    tn,
    d_model,
    tokens_in,
    mix_gain_in,
    w_query,
    w_key,
    w_value,
    w_outgate,
    w_igate_in,
    w_fgate_in,
    igate_bias_in,
    fgate_bias_in,
    head_gain_in,
    w_mixout,
    state_matrix,
    state_norm_in,
    state_max_in,
    ffn_gain_in,
    dense_mix_in,
    w_dense_gate,
    w_dense_up,
    w_dense_down,
    routes_in,
    route_weights_in,
    w_exp_gate,
    w_exp_up,
    w_exp_down,
    layer_out,
    new_matrix,
    new_norm,
    new_max,
    tokens,
    mix_gain_v,
    w_igate,
    w_fgate,
    igate_bias,
    fgate_bias,
    head_gain_v,
    state_norm,
    state_max,
    ffn_gain_v,
    dense_mix_v,
    routes,
    route_weights,
    norm_out,
    max_out,
    wq,
    wk,
    wv,
    wo,
    wm,
    sm,
    wdg,
    wdu,
    wdd,
    weg,
    weu,
    wed,
    proj_send,
    pair_proj,
    line_send,
    line_proj,
    proj_acc,
    heads_all,
    mix_send,
    mix_recv,
    hid_own,
    y_all,
    stat_send,
    stat_recv,
    stat_all,
    inv_two,
    dense_send,
    dense_recv,
    unit_all,
    exp_acc,
    res_all,
    near_recv,
    far_first,
    pair_first,
    pair_second,
    far_second,
    line_res,
    fin_send,
    fin_recv,
    fin_all,
    norm_wide,
    square,
    local_sem,
    down_sem,
    send_sem,
    recv_sem,
):
    me = lax.axis_index("ep")
    mt = lax.axis_index("tp")
    rows, feats = tokens_in.shape
    seqs = state_norm_in.shape[0]
    heads, dk, dv = sm.shape[1], sm.shape[2], sm.shape[3]
    hk, hv = heads * dk, heads * dv
    wide = 2 * hk + 2 * hv
    units = wdg.shape[1]
    quarter = rows // tn
    half = quarter // 2
    lines = n // 2
    line, side = me // 2, me % 2
    near, far, both = flip(mt, 1), flip(mt, 2), flip(mt, 3)
    started = []


    def fetch(src, dst):
        copy = pltpu.make_async_copy(src, dst, local_sem.at[len(started)])
        copy.start()
        started.append(copy)
        return copy

    first_inputs = [
        fetch(src, dst)
        for src, dst in (
            (tokens_in, tokens),
            (mix_gain_in, mix_gain_v),
            (w_igate_in, w_igate),
            (w_fgate_in, w_fgate),
            (w_query, wq),
            (w_key, wk),
            (w_value, wv),
            (w_outgate, wo),
        )
    ]

    barrier = pltpu.get_barrier_semaphore()

    def ep_flip(k):
        return flip(me, k)

    for k in range(1, n):
        pl.semaphore_signal(
            barrier, inc=1, device_id={"ep": ep_flip(k)}, device_id_type=MESH
        )
    for k in range(1, tn):
        pl.semaphore_signal(
            barrier, inc=1, device_id={"tp": flip(mt, k)}, device_id_type=MESH
        )

    in_s = fetch(state_matrix, sm)
    later_inputs = [
        fetch(src, dst)
        for src, dst in (
            (igate_bias_in, igate_bias),
            (fgate_bias_in, fgate_bias),
            (head_gain_in, head_gain_v),
            (state_norm_in, state_norm),
            (state_max_in, state_max),
            (ffn_gain_in, ffn_gain_v),
            (dense_mix_in, dense_mix_v),
            (routes_in, routes),
            (route_weights_in, route_weights),
        )
    ]
    in_m = fetch(w_mixout, wm)
    in_dg = fetch(w_dense_gate, wdg)
    in_du = fetch(w_dense_up, wdu)
    in_dd = fetch(w_dense_down, wdd)
    in_eg = fetch(w_exp_gate.at[0], weg)
    in_eu = fetch(w_exp_up.at[0], weu)

    def down_copy(t):
        src = w_exp_down.at[0, :, pl.ds(pl.multiple_of(t * feats, 128), feats)]
        return pltpu.make_async_copy(src, wed.at[t], down_sem.at[t])

    for t in range(n):
        down_copy(t).start()

    sent = []

    def remote(device, src, dst):
        at = len(sent)
        copy = pltpu.make_async_remote_copy(
            src_ref=src,
            dst_ref=dst,
            send_sem=send_sem.at[at],
            recv_sem=recv_sem.at[at],
            device_id=device,
            device_id_type=MESH,
        )
        sent.append(copy)
        copy.start()
        return copy

    def to_ep(k):
        return {"ep": ep_flip(k)}

    def to_tp(k):
        return {"tp": flip(mt, k)}

    def group(j, other):
        return flip(line, j) * 2 + (1 - side if other else side)

    def quarter_of(t):
        return pl.ds(pl.multiple_of(t * quarter, quarter), quarter)

    def half_of(t, second):
        return pl.ds(pl.multiple_of(t * quarter + second * half, half), half)

    far_lines = list(range(lines - 1, 0, -1))

    for copy in first_inputs:
        copy.wait()
    mix_gain = mix_gain_v[...].astype(F32).reshape(1, feats)
    gate_weights = jnp.concatenate(
        [w_igate[...].astype(F32), w_fgate[...].astype(F32), jnp.zeros((128 - 2 * heads, feats), F32)],
        axis=0,
    ).astype(BF16)
    tok = tokens[...].astype(F32)
    scaled = (tok * mix_gain).astype(BF16)
    squares = jnp.sum(tok * tok, axis=1, keepdims=True)

    def split_gates(total):
        high = total.astype(BF16).astype(F32)
        return (high + pltpu.roll((total - high).astype(BF16).astype(F32), 64, 1)).astype(BF16)

    lanes = lax.broadcasted_iota(jnp.int32, (rows, 128), 1)
    gates = lax.dot_general(
        scaled, gate_weights, (((1,), (1,)), ((), ())), preferred_element_type=F32
    ) + jnp.where(lanes == 2 * heads, squares, 0.0)
    proj_send[:, :, wide : wide + 128] = split_gates(gates).reshape(n, seqs, 128)
    offset = 0
    for weight in (wq, wk, wv, wo):
        width = weight.shape[1]
        part = dot(scaled, weight[...]).reshape(n, seqs, width)
        proj_send[:, :, offset : offset + width] = part.astype(BF16)
        offset += width
    pl.semaphore_wait(barrier, n + tn - 2)
    pair_copies = {
        j: remote(to_ep(1), proj_send.at[group(j, True)], pair_proj.at[j])
        for j in far_lines + [0]
    }
    line_copies = {}
    for j in far_lines:
        pair_copies[j].wait_recv()
        total = proj_send[group(j, False)].astype(F32) + pair_proj[j].astype(F32)
        line_send[j - 1, :, 0:wide] = total[:, 0:wide].astype(BF16)
        packed = total[:, wide:]
        line_send[j - 1, :, wide:] = split_gates(
            jnp.where(lanes[0:seqs] < 64, packed + pltpu.roll(packed, 64, 1), 0.0)
        )
        line_copies[j] = remote(to_ep(2 * j), line_send.at[j - 1], line_proj.at[j - 1])
    for copy in later_inputs:
        copy.wait()
    bias_lane = lax.broadcasted_iota(jnp.int32, (1, 128), 1)
    in_bias = jnp.zeros((1, 128), F32)
    forget_bias = jnp.zeros((1, 128), F32)
    for h in range(heads):
        in_bias = jnp.where(bias_lane == h, igate_bias[h], in_bias)
        forget_bias = jnp.where(bias_lane == h, fgate_bias[h], forget_bias)
    head_gain = head_gain_v[...].astype(F32).reshape(1, hv)
    ffn_gain = ffn_gain_v[...].astype(F32).reshape(1, feats)
    dense_mix = dense_mix_v[...].astype(F32).reshape(1, feats)
    pair_copies[0].wait_recv()
    proj_acc[...] = proj_send[me].astype(F32) + pair_proj[0].astype(F32)
    for j in reversed(far_lines):
        line_copies[j].wait_recv()
        proj_acc[...] += line_proj[j - 1].astype(F32)
    packed = proj_acc[:, wide:]
    gate_total = packed + pltpu.roll(packed, 64, 1)
    inverse = lax.rsqrt(pick_lane(gate_total, 2 * heads) / d_model + EPSILON)
    gate_total = gate_total * inverse
    in_log = SOFT_CAP * jnp.tanh((gate_total + in_bias) / SOFT_CAP)
    forget_pre = pltpu.roll(gate_total, 128 - heads, 1)
    capped = SOFT_CAP * jnp.tanh((forget_pre + forget_bias) / SOFT_CAP)
    forget_log = jnp.minimum(capped, 0.0) - jnp.log1p(jnp.exp(-jnp.abs(capped)))
    square[...] = jnp.zeros_like(square)
    square[0:heads, 0:seqs] = state_max[...]
    moved = forget_log + square[...].T[0:seqs, :]
    top = jnp.maximum(moved, in_log)
    carried = jnp.exp(moved - top)
    fresh = jnp.exp(in_log - top)
    floor = jnp.exp(-top)
    top_square = jnp.concatenate([top, jnp.zeros((128 - seqs, 128), F32)], axis=0).T
    max_out[...] = top_square[0:heads, 0:seqs]
    max_copy = pltpu.make_async_copy(max_out, new_max, local_sem.at[25])
    max_copy.start()
    head_lane = lax.broadcasted_iota(jnp.int32, (seqs, hk), 1) // dk
    carried_cols = [pick_lane(carried, h) for h in range(heads)]
    floor_cols = [pick_lane(floor, h) for h in range(heads)]
    carried_wide = jnp.zeros((seqs, hk), F32)
    fresh_wide = jnp.zeros((seqs, hk), F32)
    for h in range(heads):
        carried_wide = jnp.where(head_lane == h, carried_cols[h], carried_wide)
        fresh_wide = jnp.where(head_lane == h, pick_lane(fresh, h), fresh_wide)

    def rounded(lo, width):
        return (proj_acc[:, lo : lo + width] * inverse).astype(BF16).astype(F32)

    query = rounded(0, hk) * dk ** (-0.5)
    key = rounded(hk, hk) * fresh_wide
    value = rounded(2 * hk, hv)
    outgate = rounded(2 * hk + hv, hv)
    for h in range(heads):
        norm_wide[:, h * dk : (h + 1) * dk] = state_norm[:, h, :]
    norm = carried_wide * norm_wide[...] + key
    for h in range(heads):
        norm_out[:, h, :] = norm[:, h * dk : (h + 1) * dk]
    norm_copy = pltpu.make_async_copy(norm_out, new_norm, local_sem.at[26])
    norm_copy.start()
    product = norm * query
    padding = jnp.zeros((128 - seqs, hk), F32)
    query_t = jnp.concatenate([query, padding], axis=0).T
    key_t = jnp.concatenate([key, padding], axis=0).T
    in_s.wait()
    for h in range(heads):
        hs = slice(h * dk, (h + 1) * dk)
        readouts = []
        for r in range(seqs):
            state = (
                carried_cols[h][r : r + 1, :] * sm[r, h]
                + key_t[hs, r : r + 1] * value[r : r + 1, h * dv : (h + 1) * dv]
            )
            sm[r, h] = state
            readouts.append(jnp.sum(state * query_t[hs, r : r + 1], axis=0, keepdims=True))
        numerator = jnp.concatenate(readouts, axis=0)
        denominator = jnp.sum(jnp.where(head_lane == h, product, 0.0), axis=1, keepdims=True)
        readout = numerator / jnp.maximum(jnp.abs(denominator), floor_cols[h])
        cols = slice(h * dv, (h + 1) * dv)
        scale = lax.rsqrt(jnp.mean(readout * readout, axis=1, keepdims=True) + EPSILON)
        gated = readout * scale * head_gain[:, cols]
        gated = gated * jax.nn.sigmoid(outgate[:, cols])
        heads_all[me, :, cols] = gated.astype(BF16)

    heads_copies = [
        remote(to_ep(k), heads_all.at[me], heads_all.at[me]) for k in range(n - 1, 0, -1)
    ]
    state_out = pltpu.make_async_copy(sm, new_matrix, local_sem.at[27])
    state_out.start()
    in_m.wait()
    for copy in heads_copies:
        copy.wait_recv()
    mix_send[...] = dot(heads_all[...].reshape(rows, hv), wm[...]).astype(BF16)
    mix_copies = [
        remote(to_tp(k), mix_send.at[quarter_of(flip(mt, k)), :], mix_recv.at[k - 1])
        for k in range(tn - 1, 0, -1)
    ]
    mine = quarter_of(mt)
    mixed = mix_send[mine, :].astype(F32)
    for k, copy in zip(range(tn - 1, 0, -1), mix_copies):
        copy.wait_recv()
        mixed = mixed + mix_recv[k - 1].astype(F32)
    hidden = (tokens[mine, :].astype(F32) + mixed.astype(BF16).astype(F32)).astype(BF16)
    held = hidden.astype(F32)
    gained = held * ffn_gain
    y_all[me, mine, :] = gained.astype(BF16)

    def same(device, at, part):
        view = y_all.at[at, part, :]
        return remote(device, view, view)

    y_line = {j: same(to_ep(2 * j), me, mine) for j in far_lines}
    y_pair, y_far, y_near = {}, {}, {}
    y_pair_far, y_far_pair, y_pair_near, y_far_near, y_last_near = {}, {}, {}, {}, {}

    def spread(j):
        if j:
            y_line[j].wait_recv()
        y_pair[j] = same(to_ep(1), group(j, False), mine)
        y_far[j] = same(to_tp(2), group(j, False), mine)
        y_near[j] = same(to_tp(1), group(j, False), mine)

    def second(j):
        y_pair[j].wait_recv()
        y_pair_far[j] = same(to_tp(2), group(j, True), half_of(mt, 0))
        y_pair_near[j] = same(to_tp(1), group(j, True), mine)
        y_far[j].wait_recv()
        y_far_pair[j] = same(to_ep(1), group(j, False), half_of(far, 1))
        y_far_near[j] = same(to_tp(1), group(j, False), quarter_of(far))

    def third(j):
        y_pair_far[j].wait_recv()
        y_far_pair[j].wait_recv()
        y_last_near[j] = same(to_tp(1), group(j, True), quarter_of(far))

    spread(0)
    hid_own[...] = held
    squares = jnp.sum(held * held, axis=1, keepdims=True)
    gate_dot = jnp.sum(gained * dense_mix, axis=1, keepdims=True)
    lanes = lax.broadcasted_iota(jnp.int32, (quarter, 128), 1)
    stats = jnp.where(lanes == 0, squares, jnp.where(lanes == 1, gate_dot, 0.0))
    block = jnp.concatenate([stats, jnp.zeros((128 - quarter, 128), F32)], axis=0)
    stat_send[...] = block.T[0:8, :]
    stat_copies = [
        remote(to_ep(k), stat_send, stat_recv.at[k - 1]) for k in range(n - 1, 0, -1)
    ]

    def expert_block(source, first):
        feat_rows = pl.ds(pl.multiple_of(source * feats, feats), feats)
        held = y_all[source]
        for lo, weight in ((0, weg), (units, weu)):
            cols = slice(lo, lo + units)
            part = dot(held, weight[feat_rows, :])
            if first:
                exp_acc[:, cols] = part
            else:
                exp_acc[:, cols] += part

    def expert_same(j):
        y_near[j].wait_recv()
        y_far_near[j].wait_recv()
        expert_block(group(j, False), j == 0)

    def expert_other(j):
        y_pair_near[j].wait_recv()
        y_last_near[j].wait_recv()
        expert_block(group(j, True), False)

    spread(1)
    second(0)
    for j in range(2, lines):
        spread(j)
    in_dg.wait()
    in_du.wait()
    y_near[0].wait_recv()
    y_far_near[0].wait_recv()
    for lo, weight in ((0, wdg), (units, wdu)):
        part = dot(y_all[me], weight[...]).reshape(n, seqs, units)
        dense_send[:, :, lo : lo + units] = part.astype(BF16)
    dense_copies = [
        remote(to_ep(k), dense_send.at[ep_flip(k)], dense_recv.at[k - 1])
        for k in range(n - 1, 0, -1)
    ]
    in_eg.wait()
    in_eu.wait()
    expert_block(me, True)
    second(1)
    third(0)
    stat_total = stat_send[...]
    for k, copy in zip(range(n - 1, 0, -1), stat_copies):
        copy.wait_recv()
        stat_total = stat_total + stat_recv[k - 1]
    stat_all[mt] = stat_total
    stat_tp = [remote(to_tp(k), stat_all.at[mt], stat_all.at[mt]) for k in range(tn - 1, 0, -1)]
    expert_same(1)
    expert_other(0)
    for j in range(2, lines):
        second(j)
        third(j - 1)
        expert_same(j)
        expert_other(j - 1)
    third(lines - 1)
    for copy in stat_tp:
        copy.wait_recv()
    for q in range(tn):
        columns = jnp.concatenate([stat_all[q], jnp.zeros((120, 128), F32)], axis=0).T
        scale = lax.rsqrt(pick_lane(columns, 0) / d_model + EPSILON)
        inv_two[q * quarter : (q + 1) * quarter, :] = jnp.broadcast_to(scale, (128, 128))[0:quarter]
    dense_total = dense_send[me].astype(F32)
    for k, copy in zip(range(n - 1, 0, -1), dense_copies):
        copy.wait_recv()
        dense_total = dense_total + dense_recv[k - 1].astype(F32)
    seq_scale = inv_two[pl.ds(pl.multiple_of(me * seqs, seqs), seqs), 0:1]
    dense_total = dense_total * seq_scale
    unit_all[me] = (
        jax.nn.silu(dense_total[:, 0:units]) * dense_total[:, units : 2 * units]
    ).astype(BF16)
    unit_copies = [
        remote(to_ep(k), unit_all.at[me], unit_all.at[me]) for k in range(n - 1, 0, -1)
    ]
    expert_other(lines - 1)
    picks = routes[...] == me
    weight = jnp.sum(jnp.where(picks, route_weights[...], 0.0), axis=0, keepdims=True)
    weight = pick_lane(jnp.broadcast_to(weight, (rows, rows)).T, 0)
    scale = inv_two[:, 0:1]
    gate = exp_acc[:, 0:units] * scale
    up = exp_acc[:, units : 2 * units] * scale
    expert_units = (jax.nn.silu(gate) * up * weight).astype(BF16)

    near_copies, far_a, pair_b, pair_a, far_b, line_out = {}, {}, {}, {}, {}, {}

    def compute(j):
        near_copies[j] = []
        for other in (True, False):
            t = group(j, other)
            down_copy(t).wait()
            res_all[t] = dot(expert_units, wed[t]).astype(BF16)
            for slot, q in ((1, both), (0, near)):
                near_copies[j].append(
                    remote(
                        to_tp(1),
                        res_all.at[t, quarter_of(q), :],
                        near_recv.at[2 * j + other, slot],
                    )
                )

    def add(at, part, other):
        total = res_all[at, part, :].astype(F32) + other.astype(F32)
        res_all[at, part, :] = total.astype(BF16)

    def first_sums(j):
        for copy in near_copies[j]:
            copy.wait_recv()
        far_a[j], pair_b[j] = [], []
        for other in (True, False):
            t = group(j, other)
            add(t, quarter_of(far), near_recv[2 * j + other, 1])
            add(t, mine, near_recv[2 * j + other, 0])
            far_a[j].append(
                remote(to_tp(2), res_all.at[t, half_of(far, 0), :], far_first.at[2 * j + other])
            )
            if other:
                for slot, q in ((1, far), (0, mt)):
                    pair_b[j].append(
                        remote(
                            to_ep(1), res_all.at[t, half_of(q, 1), :], pair_first.at[j, slot]
                        )
                    )

    def second_sums(j):
        for copy in far_a[j]:
            copy.wait_recv()
        add(group(j, True), half_of(mt, 0), far_first[2 * j + 1])
        pair_a[j] = remote(
            to_ep(1), res_all.at[group(j, True), half_of(mt, 0), :], pair_second.at[j]
        )
        add(group(j, False), half_of(mt, 0), far_first[2 * j])
        for copy in pair_b[j]:
            copy.wait_recv()
        add(group(j, False), half_of(far, 1), pair_first[j, 1])
        far_b[j] = remote(
            to_tp(2), res_all.at[group(j, False), half_of(far, 1), :], far_second.at[j]
        )
        add(group(j, False), half_of(mt, 1), pair_first[j, 0])

    def third_sums(j):
        pair_a[j].wait_recv()
        add(group(j, False), half_of(mt, 0), pair_second[j])
        far_b[j].wait_recv()
        add(group(j, False), half_of(mt, 1), far_second[j])
        if j:
            line_out[j] = remote(
                to_ep(2 * j), res_all.at[group(j, False), mine, :], line_res.at[j - 1]
            )

    order = far_lines + [0]
    for j in order:
        compute(j)
    for j in order:
        first_sums(j)
    for j in order[:-1]:
        second_sums(j)
    in_dd.wait()
    for copy in unit_copies:
        copy.wait_recv()
    fin_send[...] = dot(unit_all[...].reshape(rows, units), wdd[...]).astype(BF16)
    fin_copies = [
        remote(to_tp(k), fin_send.at[quarter_of(flip(mt, k)), :], fin_recv.at[k - 1])
        for k in range(tn - 1, 0, -1)
    ]
    third_sums(order[0])
    second_sums(0)
    for j in order[1:]:
        third_sums(j)
    dense = fin_send[mine, :].astype(F32)
    for k, copy in zip(range(tn - 1, 0, -1), fin_copies):
        copy.wait_recv()
        dense = dense + fin_recv[k - 1].astype(F32)
    columns = jnp.concatenate([stat_total, jnp.zeros((120, 128), F32)], axis=0).T
    scale = lax.rsqrt(pick_lane(columns, 0) / d_model + EPSILON)
    gate = jax.nn.sigmoid(scale * pick_lane(columns, 1))[0:quarter]
    total = hid_own[...] + res_all[me, mine, :].astype(F32) + gate * dense
    for j in far_lines:
        line_out[j].wait_recv()
        total = total + line_res[j - 1].astype(F32)
    fin_all[mine, :] = total.astype(BF16)
    all_copies = [
        remote(to_tp(k), fin_all.at[mine, :], fin_all.at[mine, :]) for k in range(tn - 1, 0, -1)
    ]
    outs = []

    def write(at, t):
        copy = pltpu.make_async_copy(
            fin_all.at[quarter_of(t), :], layer_out.at[quarter_of(t), :], local_sem.at[28 + at]
        )
        copy.start()
        outs.append(copy)

    write(0, mt)
    for k, copy in zip(range(tn - 1, 0, -1), all_copies):
        copy.wait_recv()
        write(k, flip(mt, k))
    max_copy.wait()
    norm_copy.wait()
    state_out.wait()
    for copy in sent:
        copy.wait_send()
    for copy in outs:
        copy.wait()


def finish_kernel(parts, layer_in, matrix_in, norm_in, max_in, layer_out, matrix_out, norm_out, max_out, layer_v, matrix_v, norm_v, max_v, in_sem, out_sem):
    seqs = matrix_in.shape[0] // parts
    pairs = [
        (matrix_in.at[pl.ds(i * seqs, seqs)], matrix_v.at[pl.ds(i * seqs, seqs)], matrix_out.at[pl.ds(i * seqs, seqs)])
        for i in range(parts)
    ] + [(layer_in, layer_v, layer_out), (norm_in, norm_v, norm_out), (max_in, max_v, max_out)]
    into = [pltpu.make_async_copy(src, held, in_sem.at[i]) for i, (src, held, _) in enumerate(pairs)]
    out = [pltpu.make_async_copy(held, dst, out_sem.at[i]) for i, (_, held, dst) in enumerate(pairs)]
    for copy in into:
        copy.start()
    for first, second in zip(into, out):
        first.wait()
        second.start()
    for copy in out:
        copy.wait()


def finish(layer_out, new_matrix, new_norm, new_max):
    parts = 8
    arrays = (layer_out, new_matrix, new_norm, new_max)
    hbm = pl.BlockSpec(memory_space=pl.ANY)
    return pl.pallas_call(
        functools.partial(finish_kernel, parts),
        out_shape=tuple(jax.ShapeDtypeStruct(a.shape, a.dtype) for a in arrays),
        in_specs=[hbm] * 4,
        out_specs=(hbm,) * 4,
        scratch_shapes=[pltpu.VMEM(a.shape, a.dtype) for a in arrays]
        + [pltpu.SemaphoreType.DMA((parts + 3,)), pltpu.SemaphoreType.DMA((parts + 3,))],
        compiler_params=pltpu.CompilerParams(vmem_limit_bytes=66_900_000),
    )(*arrays)

def on_device(
    n,
    tn,
    tokens,
    mix_gain,
    w_query,
    w_key,
    w_value,
    w_outgate,
    w_igate,
    w_fgate,
    igate_bias,
    fgate_bias,
    head_gain,
    w_mixout,
    state_matrix,
    state_norm,
    state_max,
    ffn_gain,
    dense_mix,
    w_dense_gate,
    w_dense_up,
    w_dense_down,
    routes,
    route_weights,
    w_exp_gate,
    w_exp_up,
    w_exp_down,
):
    rows, feats = tokens.shape
    seqs, heads, dk, dv = state_matrix.shape
    hk, hv = heads * dk, heads * dv
    units = w_dense_gate.shape[1]
    wide = 2 * hk + 2 * hv
    quarter = rows // tn
    hbm = pl.BlockSpec(memory_space=pl.ANY)
    dma = pltpu.SemaphoreType.DMA
    lines, half = n // 2, quarter // 2
    scratch = [
        pltpu.VMEM(tokens.shape, BF16),
        pltpu.VMEM(mix_gain.shape, BF16),
        pltpu.VMEM((heads, feats), BF16),
        pltpu.VMEM((heads, feats), BF16),
        pltpu.SMEM(igate_bias.shape, F32),
        pltpu.SMEM(fgate_bias.shape, F32),
        pltpu.VMEM(head_gain.shape, BF16),
        pltpu.VMEM(state_norm.shape, F32),
        pltpu.VMEM((heads, seqs), F32),
        pltpu.VMEM(ffn_gain.shape, BF16),
        pltpu.VMEM(dense_mix.shape, BF16),
        pltpu.VMEM((routes.shape[1], rows), jnp.int32),
        pltpu.VMEM((routes.shape[1], rows), F32),
        pltpu.VMEM(state_norm.shape, F32),
        pltpu.VMEM((heads, seqs), F32),
        pltpu.VMEM(w_query.shape, BF16),
        pltpu.VMEM(w_key.shape, BF16),
        pltpu.VMEM(w_value.shape, BF16),
        pltpu.VMEM(w_outgate.shape, BF16),
        pltpu.VMEM(w_mixout.shape, BF16),
        pltpu.VMEM(state_matrix.shape, F32),
        pltpu.VMEM(w_dense_gate.shape, BF16),
        pltpu.VMEM(w_dense_up.shape, BF16),
        pltpu.VMEM(w_dense_down.shape, BF16),
        pltpu.VMEM(w_exp_gate.shape[1:], BF16),
        pltpu.VMEM(w_exp_up.shape[1:], BF16),
        pltpu.VMEM((n, units, feats), BF16),
        pltpu.VMEM((n, seqs, wide + 128), BF16),
        pltpu.VMEM((lines, seqs, wide + 128), BF16),
        pltpu.VMEM((lines - 1, seqs, wide + 128), BF16),
        pltpu.VMEM((lines - 1, seqs, wide + 128), BF16),
        pltpu.VMEM((seqs, wide + 128), F32),
        pltpu.VMEM((n, seqs, hv), BF16),
        pltpu.VMEM((rows, feats), BF16),
        pltpu.VMEM((tn - 1, quarter, feats), BF16),
        pltpu.VMEM((quarter, feats), F32),
        pltpu.VMEM((n, rows, feats), BF16),
        pltpu.VMEM((8, 128), F32),
        pltpu.VMEM((n - 1, 8, 128), F32),
        pltpu.VMEM((tn, 8, 128), F32),
        pltpu.VMEM((rows, 128), F32),
        pltpu.VMEM((n, seqs, 2 * units), BF16),
        pltpu.VMEM((n - 1, seqs, 2 * units), BF16),
        pltpu.VMEM((n, seqs, units), BF16),
        pltpu.VMEM((rows, 2 * units), F32),
        pltpu.VMEM((n, rows, feats), BF16),
        pltpu.VMEM((n, 2, quarter, feats), BF16),
        pltpu.VMEM((n, half, feats), BF16),
        pltpu.VMEM((lines, 2, half, feats), BF16),
        pltpu.VMEM((lines, half, feats), BF16),
        pltpu.VMEM((lines, half, feats), BF16),
        pltpu.VMEM((lines - 1, quarter, feats), BF16),
        pltpu.VMEM((rows, feats), BF16),
        pltpu.VMEM((tn - 1, quarter, feats), BF16),
        pltpu.VMEM((rows, feats), BF16),
        pltpu.VMEM((seqs, hk), F32),
        pltpu.VMEM((128, 128), F32),
        dma((32,)),
        dma((n,)),
        dma((160,)),
        dma((160,)),
    ]
    layer_out, new_matrix, new_norm, new_max = pl.pallas_call(
        functools.partial(layer_kernel, n, tn, n * feats),
        out_shape=(
            jax.ShapeDtypeStruct((rows, feats), BF16),
            jax.ShapeDtypeStruct(state_matrix.shape, F32),
            jax.ShapeDtypeStruct(state_norm.shape, F32),
            jax.ShapeDtypeStruct((heads, seqs), F32),
        ),
        in_specs=[hbm] * 25,
        out_specs=(hbm,) * 4,
        scratch_shapes=scratch,
        compiler_params=pltpu.CompilerParams(
            collective_id=0, has_side_effects=True, vmem_limit_bytes=66_900_000
        ),
    )(
        tokens,
        mix_gain,
        w_query,
        w_key,
        w_value,
        w_outgate,
        w_igate.T,
        w_fgate.T,
        igate_bias,
        fgate_bias,
        head_gain,
        w_mixout,
        state_matrix,
        state_norm,
        state_max.T,
        ffn_gain,
        dense_mix,
        w_dense_gate,
        w_dense_up,
        w_dense_down,
        routes.T,
        route_weights.T,
        w_exp_gate,
        w_exp_up,
        w_exp_down,
    )
    layer_out, new_matrix, new_norm, new_max = finish(layer_out, new_matrix, new_norm, new_max)
    return layer_out, new_matrix, new_norm, new_max.T


def wide_kernel(
    n,
    tn,
    d_model,
    tokens,
    small,
    w_gates,
    state_norm,
    state_max,
    routes,
    route_weights,
    w_query,
    w_key,
    w_value,
    w_outgate,
    w_mixout,
    state_matrix,
    w_dense_gate,
    w_dense_up,
    w_dense_down,
    w_exp_gate,
    w_exp_up,
    w_exp_down,
    layer_out,
    new_matrix,
    new_norm,
    new_max,
    wq,
    wk,
    wv,
    wo,
    wm,
    sm,
    wdg,
    wdu,
    wdd,
    weg,
    weu,
    wed,
    proj_send,
    proj_recv,
    gate_send,
    gate_recv,
    num,
    heads_all,
    mix_send,
    mix_recv,
    hid_own,
    y_all,
    stat_send,
    stat_recv,
    stat_all,
    inv_two,
    dense_send,
    dense_recv,
    unit_all,
    exp_acc,
    near_recv,
    far_recv,
    res_recv,
    out_acc,
    fin_send,
    fin_recv,
    fin_all,
    norm_wide,
    square,
    local_sem,
    down_sem,
    ep_send,
    ep_recv,
    tp_send,
    tp_recv,
    pair_send,
    pair_recv,
):
    me = lax.axis_index("ep")
    mt = lax.axis_index("tp")
    rows, feats = tokens.shape
    chunk = min(rows, 128)
    chunks = rows // chunk
    seqs = state_norm.shape[0]
    heads, dk, dv = sm.shape[1], sm.shape[2], sm.shape[3]
    hk, hv = heads * dk, heads * dv
    units = wdg.shape[1]
    quarter = rows // tn
    per_chunk = chunk // seqs

    def fetch(i, src, dst):
        copy = pltpu.make_async_copy(src, dst, local_sem.at[i])
        copy.start()
        return copy

    in_q = fetch(0, w_query, wq)
    in_k = fetch(1, w_key, wk)
    in_v = fetch(2, w_value, wv)
    in_o = fetch(3, w_outgate, wo)
    in_s = fetch(4, state_matrix, sm)
    in_m = fetch(5, w_mixout, wm)
    in_dg = fetch(6, w_dense_gate, wdg)
    in_du = fetch(7, w_dense_up, wdu)
    in_dd = fetch(8, w_dense_down, wdd)
    in_eg = fetch(9, w_exp_gate.at[0], weg)
    in_eu = fetch(10, w_exp_up.at[0], weu)

    def down_copy(t):
        if w_exp_down.shape[2] == n * feats:
            src = w_exp_down.at[0, :, pl.ds(pl.multiple_of(t * feats, 128), feats)]
        else:
            src = w_exp_down.at[t]
        return pltpu.make_async_copy(src, wed.at[t], down_sem.at[t])

    each(n, lambda t: down_copy(t).start())

    def ep_copy(phase, k, src, dst):
        return pltpu.make_async_remote_copy(
            src_ref=src,
            dst_ref=dst,
            send_sem=ep_send.at[phase, k - 1],
            recv_sem=ep_recv.at[phase, k - 1],
            device_id={"ep": lax.rem(me + k, n)},
            device_id_type=MESH,
        )

    def tp_copy(phase, k, src, dst):
        return pltpu.make_async_remote_copy(
            src_ref=src,
            dst_ref=dst,
            send_sem=tp_send.at[phase, k - 1],
            recv_sem=tp_recv.at[phase, k - 1],
            device_id={"tp": lax.rem(mt + k, tn)},
            device_id_type=MESH,
        )

    def peers(body):
        each(n - 1, lambda i: body(i + 1))

    def tp_peers(body):
        each(tn - 1, lambda i: body(i + 1))

    barrier = pltpu.get_barrier_semaphore()
    peers(
        lambda k: pl.semaphore_signal(
            barrier, inc=1, device_id={"ep": lax.rem(me + k, n)}, device_id_type=MESH
        )
    )
    tp_peers(
        lambda k: pl.semaphore_signal(
            barrier, inc=1, device_id={"tp": lax.rem(mt + k, tn)}, device_id_type=MESH
        )
    )

    def row_slice(c):
        return pl.ds(pl.multiple_of(c * chunk, chunk), chunk)

    in_q.wait()
    in_k.wait()
    in_v.wait()
    in_o.wait()

    def project(c):
        tok = tokens[row_slice(c), :].astype(F32)
        scaled = (tok * small[0:1, 0:feats]).astype(BF16)
        squares = jnp.sum(tok * tok, axis=1, keepdims=True)
        blocks = pl.ds(c * per_chunk, per_chunk)
        lanes = lax.broadcasted_iota(jnp.int32, (chunk, 128), 1)
        gates = lax.dot_general(
            scaled, w_gates[...], (((1,), (1,)), ((), ())), preferred_element_type=F32
        ) + jnp.where(lanes == 2 * heads, squares, 0.0)
        gate_send[blocks] = gates.reshape(per_chunk, seqs, 128)
        offset = 0
        for weight in (wq, wk, wv, wo):
            width = weight.shape[1]
            part = dot(scaled, weight[...]).reshape(per_chunk, seqs, width)
            proj_send[blocks, :, offset : offset + width] = part.astype(BF16)
            offset += width

    each(chunks, project)
    pl.semaphore_wait(barrier, n + tn - 2)

    def proj_copy(k):
        t = lax.rem(me + k, n)
        return ep_copy(0, k, proj_send.at[t], proj_recv.at[k - 1])

    def gate_copy(k):
        t = lax.rem(me + k, n)
        return ep_copy(1, k, gate_send.at[t], gate_recv.at[k - 1])

    peers(lambda k: (gate_copy(k).start(), proj_copy(k).start()))

    proj_acc = num
    gate_total = gate_send[me]
    proj_acc[...] = proj_send[me].astype(F32)
    if n <= 8:
        for k in range(1, n):
            gate_copy(k).wait_recv()
            gate_total = gate_total + gate_recv[k - 1]
    else:
        peers(lambda k: gate_copy(k).wait_recv())
        gate_total = lax.fori_loop(1, n, lambda k, acc: acc + gate_recv[k - 1], gate_total)

    def take_proj(k):
        proj_copy(k).wait_recv()
        proj_acc[...] += proj_recv[k - 1].astype(F32)

    inverse = lax.rsqrt(pick_lane(gate_total, 2 * heads) / d_model + EPSILON)
    gate_total = gate_total * inverse
    in_log = SOFT_CAP * jnp.tanh((gate_total + small[4:5, 0:128]) / SOFT_CAP)
    forget_pre = pltpu.roll(gate_total, 128 - heads, 1)
    capped = SOFT_CAP * jnp.tanh((forget_pre + small[5:6, 0:128]) / SOFT_CAP)
    forget_log = jnp.minimum(capped, 0.0) - jnp.log1p(jnp.exp(-jnp.abs(capped)))
    square[...] = jnp.zeros_like(square)
    square[0:heads, 0:seqs] = state_max[...]
    moved = forget_log + square[...].T[0:seqs, :]
    top = jnp.maximum(moved, in_log)
    carried = jnp.exp(moved - top)
    fresh = jnp.exp(in_log - top)
    floor = jnp.exp(-top)
    top_square = jnp.concatenate([top, jnp.zeros((128 - seqs, 128), F32)], axis=0).T
    new_max[...] = top_square[0:heads, 0:seqs]
    head_lane = lax.broadcasted_iota(jnp.int32, (seqs, hk), 1) // dk
    carried_cols = [pick_lane(carried, h) for h in range(heads)]
    floor_cols = [pick_lane(floor, h) for h in range(heads)]
    carried_wide = jnp.zeros((seqs, hk), F32)
    fresh_wide = jnp.zeros((seqs, hk), F32)
    for h in range(heads):
        carried_wide = jnp.where(head_lane == h, carried_cols[h], carried_wide)
        fresh_wide = jnp.where(head_lane == h, pick_lane(fresh, h), fresh_wide)

    peers(take_proj)

    def rounded(lo, width):
        return (proj_acc[:, lo : lo + width] * inverse).astype(BF16).astype(F32)

    query = rounded(0, hk) * dk ** (-0.5)
    key = rounded(hk, hk) * fresh_wide
    value = rounded(2 * hk, hv)
    outgate = rounded(2 * hk + hv, hv)
    for h in range(heads):
        norm_wide[:, h * dk : (h + 1) * dk] = state_norm[:, h, :]
    norm = carried_wide * norm_wide[...] + key
    new_norm[...] = norm
    product = norm * query
    padding = jnp.zeros((128 - seqs, hk), F32)
    query_t = jnp.concatenate([query, padding], axis=0).T
    key_t = jnp.concatenate([key, padding], axis=0).T
    in_s.wait()
    for h in range(heads):
        hs = slice(h * dk, (h + 1) * dk)
        readouts = []
        for r in range(seqs):
            state = (
                carried_cols[h][r : r + 1, :] * sm[r, h]
                + key_t[hs, r : r + 1] * value[r : r + 1, h * dv : (h + 1) * dv]
            )
            sm[r, h] = state
            readouts.append(jnp.sum(state * query_t[hs, r : r + 1], axis=0, keepdims=True))
        numerator = jnp.concatenate(readouts, axis=0)
        denominator = jnp.sum(jnp.where(head_lane == h, product, 0.0), axis=1, keepdims=True)
        readout = numerator / jnp.maximum(jnp.abs(denominator), floor_cols[h])
        cols = slice(h * dv, (h + 1) * dv)
        scale = lax.rsqrt(jnp.mean(readout * readout, axis=1, keepdims=True) + EPSILON)
        gated = readout * scale * small[3:4, cols]
        gated = gated * jax.nn.sigmoid(outgate[:, cols])
        heads_all[me, :, cols] = gated.astype(BF16)

    def heads_copy(k):
        return ep_copy(2, k, heads_all.at[me], heads_all.at[me])

    peers(lambda k: heads_copy(k).start())
    state_out = pltpu.make_async_copy(sm, new_matrix, local_sem.at[11])
    state_out.start()

    in_m.wait()
    peers(lambda k: heads_copy(k).wait_recv())

    def mix_rows(c):
        held = heads_all[pl.ds(c * per_chunk, per_chunk)].reshape(chunk, hv)
        mix_send[row_slice(c), :] = dot(held, wm[...]).astype(BF16)

    each(chunks, mix_rows)

    def quarter_of(t):
        return pl.ds(pl.multiple_of(t * quarter, quarter), quarter)

    def mix_copy(k):
        return tp_copy(
            0, k, mix_send.at[quarter_of(lax.rem(mt + k, tn)), :], mix_recv.at[k - 1]
        )

    tp_peers(lambda k: mix_copy(k).start())
    mine = quarter_of(mt)
    near = mt + 1 - 2 * lax.rem(mt, 2)
    far = lax.rem(mt + 2, tn)
    both = lax.rem(near + 2, tn)
    mixed = mix_send[mine, :].astype(F32)
    for k in range(1, tn):
        mix_copy(k).wait_recv()
        mixed = mixed + mix_recv[k - 1].astype(F32)
    hidden = (tokens[mine, :].astype(F32) + mixed.astype(BF16).astype(F32)).astype(BF16)
    held = hidden.astype(F32)
    hid_own[...] = held
    gained = held * small[1:2, 0:feats]
    y_all[me, mine, :] = gained.astype(BF16)
    squares = jnp.sum(held * held, axis=1, keepdims=True)
    gate_dot = jnp.sum(gained * small[2:3, 0:feats], axis=1, keepdims=True)
    piece = min(quarter, 128)
    pieces = quarter // piece
    lanes = lax.broadcasted_iota(jnp.int32, (quarter, 128), 1)
    stats = jnp.where(lanes == 0, squares, jnp.where(lanes == 1, gate_dot, 0.0))
    for j in range(pieces):
        block = stats[j * piece : (j + 1) * piece, :]
        if piece < 128:
            block = jnp.concatenate([block, jnp.zeros((128 - piece, 128), F32)], axis=0)
        stat_send[j] = block.T[0:8, :]

    def part_copy(partner, sems, k, src, dst):
        return pltpu.make_async_remote_copy(
            src_ref=src,
            dst_ref=dst,
            send_sem=pair_send.at[sems, k],
            recv_sem=pair_recv.at[sems, k],
            device_id={"tp": partner},
            device_id_type=MESH,
        )

    def source_of(k):
        return lax.rem(me + n - k, n)

    def target_of(k):
        return lax.rem(me + k, n)

    def y_copy(k):
        return ep_copy(3, k, y_all.at[me, mine, :], y_all.at[me, mine, :])

    def spread(partner, sems, k, rows_at):
        view = y_all.at[source_of(k), quarter_of(rows_at), :]
        return part_copy(partner, sems, k, view, view)

    def y_far(k):
        return spread(far, 0, k, mt)

    def y_near(k):
        return spread(near, 1, k, mt)

    def y_near_far(k):
        return spread(near, 2, k, far)

    def stat_copy(k):
        return ep_copy(4, k, stat_send, stat_recv.at[k - 1])

    def stat_tp(k):
        return tp_copy(1, k, stat_all.at[mt], stat_all.at[mt])

    def dense_copy(k):
        return ep_copy(5, k, dense_send.at[target_of(k)], dense_recv.at[k - 1])

    y_far(0).start()
    peers(lambda k: (stat_copy(k).start(), y_copy(k).start()))
    y_near(0).start()
    y_far(0).wait_recv()
    y_near_far(0).start()
    in_dg.wait()
    in_du.wait()
    y_near(0).wait_recv()
    y_near_far(0).wait_recv()

    def dense_rows(c):
        held = y_all[me, row_slice(c), :]
        blocks = pl.ds(c * per_chunk, per_chunk)
        for lo, weight in ((0, wdg), (units, wdu)):
            part = dot(held, weight[...]).reshape(per_chunk, seqs, units)
            dense_send[blocks, :, lo : lo + units] = part.astype(BF16)

    each(chunks, dense_rows)
    peers(lambda k: dense_copy(k).start())

    if n <= 8:
        stat_total = stat_send[...]
        for k in range(1, n):
            stat_copy(k).wait_recv()
            stat_total = stat_total + stat_recv[k - 1]
    else:
        peers(lambda k: stat_copy(k).wait_recv())
        stat_total = lax.fori_loop(1, n, lambda k, acc: acc + stat_recv[k - 1], stat_send[...])
    stat_all[mt] = stat_total
    tp_peers(lambda k: stat_tp(k).start())

    in_eg.wait()
    in_eu.wait()

    def expert_block(source, first):
        feat_rows = pl.ds(pl.multiple_of(source * feats, feats), feats)

        def body(c):
            held = y_all[source, row_slice(c), :]
            for lo, weight in ((0, weg), (units, weu)):
                cols = slice(lo, lo + units)
                part = dot(held, weight[feat_rows, :])
                if first:
                    exp_acc[row_slice(c), cols] = part
                else:
                    exp_acc[row_slice(c), cols] += part

        each(chunks, body)

    def forward(k):
        y_copy(k).wait_recv()
        y_far(k).start()
        y_near(k).start()

    def forward_far(k):
        y_far(k).wait_recv()
        y_near_far(k).start()

    def expert_step(k):
        y_near(k).wait_recv()
        y_near_far(k).wait_recv()
        expert_block(source_of(k), False)

    def staged(stages, least):
        if n <= 8:
            for i in range(least, n + len(stages) - 1):
                for late, stage in enumerate(stages):
                    if least <= i - late < n:
                        stage(i - late)
        else:
            for stage in stages:
                each(n - least, lambda i, stage=stage: stage(i + least))

    expert_block(me, True)
    staged((forward, forward_far, expert_step), 1)

    tp_peers(lambda k: stat_tp(k).wait_recv())
    for q in range(tn):
        for j in range(pieces):
            total = stat_all[q, j]
            columns = jnp.concatenate([total, jnp.zeros((120, 128), F32)], axis=0).T
            scale = lax.rsqrt(pick_lane(columns, 0) / d_model + EPSILON)
            at = q * quarter + j * piece
            inv_two[at : at + piece, :] = jnp.broadcast_to(scale, (128, 128))[0:piece]

    dense_total = dense_send[me].astype(F32)
    if n <= 8:
        for k in range(1, n):
            dense_copy(k).wait_recv()
            dense_total = dense_total + dense_recv[k - 1].astype(F32)
    else:
        peers(lambda k: dense_copy(k).wait_recv())
        dense_total = lax.fori_loop(
            1, n, lambda k, acc: acc + dense_recv[k - 1].astype(F32), dense_total
        )
    seq_scale = inv_two[pl.ds(pl.multiple_of(me * seqs, seqs), seqs), 0:1]
    dense_total = dense_total * seq_scale
    unit_all[me] = (
        jax.nn.silu(dense_total[:, 0:units]) * dense_total[:, units : 2 * units]
    ).astype(BF16)

    def unit_copy(k):
        return ep_copy(6, k, unit_all.at[me], unit_all.at[me])

    peers(lambda k: unit_copy(k).start())

    def expert_units(c):
        picks = routes[:, row_slice(c)] == me
        weight = jnp.sum(
            jnp.where(picks, route_weights[:, row_slice(c)], 0.0), axis=0, keepdims=True
        )
        weight = pick_lane(jnp.broadcast_to(weight, (chunk, chunk)).T, 0)
        scale = inv_two[row_slice(c), 0:1]
        gate = exp_acc[row_slice(c), 0:units] * scale
        up = exp_acc[row_slice(c), units : 2 * units] * scale
        exp_acc[row_slice(c), 0:units] = jax.nn.silu(gate) * up * weight

    each(chunks, expert_units)
    peers(lambda k: y_copy(k).wait_send())
    each(n, lambda k: (y_far(k).wait_send(), y_near(k).wait_send()))
    each(n, lambda k: y_near_far(k).wait_send())

    def result_view(k, rows_at):
        return y_all.at[target_of(k), quarter_of(rows_at), :]

    def res_near(k):
        return part_copy(near, 3, k, result_view(k, near), near_recv.at[k, 0])

    def res_near_far(k):
        return part_copy(near, 4, k, result_view(k, both), near_recv.at[k, 1])

    def res_far(k):
        return part_copy(far, 5, k, result_view(k, far), far_recv.at[k])

    def res_copy(k):
        return ep_copy(7, k, result_view(k, mt), res_recv.at[k - 1])

    def result_step(k):
        t = target_of(k)
        down_copy(t).wait()

        def body(c):
            held = exp_acc[row_slice(c), 0:units].astype(BF16)
            y_all[t, row_slice(c), :] = dot(held, wed[t]).astype(BF16)

        each(chunks, body)
        res_near_far(k).start()
        res_near(k).start()

    def result_far(k):
        res_near_far(k).wait_recv()
        summed = y_all[target_of(k), quarter_of(far), :].astype(F32) + near_recv[k, 1].astype(F32)
        y_all[target_of(k), quarter_of(far), :] = summed.astype(BF16)
        res_far(k).start()

    def result_sum(k):
        res_near(k).wait_recv()
        res_far(k).wait_recv()
        return (
            y_all[target_of(k), mine, :].astype(F32)
            + near_recv[k, 0].astype(F32)
            + far_recv[k].astype(F32)
        )

    def result_out(k):
        y_all[target_of(k), mine, :] = result_sum(k).astype(BF16)
        res_copy(k).start()

    staged((result_step, result_far, result_out), 1)

    result_step(0)
    in_dd.wait()
    peers(lambda k: unit_copy(k).wait_recv())

    def down_rows(c):
        hidden_units = unit_all[pl.ds(c * per_chunk, per_chunk)].reshape(chunk, units)
        fin_send[row_slice(c), :] = dot(hidden_units, wdd[...]).astype(BF16)

    each(chunks, down_rows)

    def fin_copy(k):
        return tp_copy(
            2, k, fin_send.at[quarter_of(lax.rem(mt + k, tn)), :], fin_recv.at[k - 1]
        )

    tp_peers(lambda k: fin_copy(k).start())
    result_far(0)
    dense = fin_send[mine, :].astype(F32)
    for k in range(1, tn):
        fin_copy(k).wait_recv()
        dense = dense + fin_recv[k - 1].astype(F32)
    gates = []
    for j in range(pieces):
        columns = jnp.concatenate([stat_total[j], jnp.zeros((120, 128), F32)], axis=0).T
        scale = lax.rsqrt(pick_lane(columns, 0) / d_model + EPSILON)
        gates.append(jax.nn.sigmoid(scale * pick_lane(columns, 1))[0:piece])
    gate = gates[0] if pieces == 1 else jnp.concatenate(gates, axis=0)
    out_acc[...] = result_sum(0) + gate * dense

    def take_result(k):
        res_copy(k).wait_recv()
        out_acc[...] += res_recv[k - 1].astype(F32)

    peers(take_result)
    fin_all[mine, :] = (hid_own[...] + out_acc[...]).astype(BF16)

    def all_copy(k):
        return tp_copy(3, k, fin_all.at[mine, :], fin_all.at[mine, :])

    tp_peers(lambda k: all_copy(k).start())
    tp_peers(lambda k: all_copy(k).wait_recv())
    layer_out[...] = fin_all[...]
    state_out.wait()
    for copies in (
        proj_copy,
        gate_copy,
        heads_copy,
        stat_copy,
        dense_copy,
        unit_copy,
        res_copy,
    ):
        peers(lambda k, copies=copies: copies(k).wait_send())
    for copies in (res_near, res_near_far, res_far):
        each(n, lambda k, copies=copies: copies(k).wait_send())
    for copies in (mix_copy, stat_tp, fin_copy, all_copy):
        tp_peers(lambda k, copies=copies: copies(k).wait_send())


def wide_on_device(
    n,
    tn,
    tokens,
    mix_gain,
    w_query,
    w_key,
    w_value,
    w_outgate,
    w_igate,
    w_fgate,
    igate_bias,
    fgate_bias,
    head_gain,
    w_mixout,
    state_matrix,
    state_norm,
    state_max,
    ffn_gain,
    dense_mix,
    w_dense_gate,
    w_dense_up,
    w_dense_down,
    routes,
    route_weights,
    w_exp_gate,
    w_exp_up,
    w_exp_down,
):
    rows, feats = tokens.shape
    seqs, heads, dk, dv = state_matrix.shape
    hk, hv = heads * dk, heads * dv
    units = w_dense_gate.shape[1]
    wide = 2 * hk + 2 * hv
    quarter = rows // tn
    pieces = max(1, quarter // 128)
    w_gates = jnp.pad(
        jnp.concatenate([w_igate.T, w_fgate.T], axis=0), ((0, 128 - 2 * heads), (0, 0))
    )
    width = max(feats, hv, 128)
    row_at = lax.broadcasted_iota(jnp.int32, (8, width), 0)
    small = jnp.zeros((8, width), F32)
    for at, row in enumerate(
        (mix_gain, ffn_gain, dense_mix, head_gain, igate_bias, fgate_bias)
    ):
        wide_row = jnp.pad(row.astype(F32), (0, width - row.shape[0]))
        small = jnp.where(row_at == at, wide_row[None, :], small)
    down = w_exp_down
    if feats % 128:
        down = w_exp_down[0].reshape(units, n, feats).transpose(1, 0, 2)
    vmem = pl.BlockSpec(memory_space=pltpu.VMEM)
    hbm = pl.BlockSpec(memory_space=pl.ANY)
    dma = pltpu.SemaphoreType.DMA
    scratch = [
        pltpu.VMEM(w_query.shape, BF16),
        pltpu.VMEM(w_key.shape, BF16),
        pltpu.VMEM(w_value.shape, BF16),
        pltpu.VMEM(w_outgate.shape, BF16),
        pltpu.VMEM(w_mixout.shape, BF16),
        pltpu.VMEM(state_matrix.shape, F32),
        pltpu.VMEM(w_dense_gate.shape, BF16),
        pltpu.VMEM(w_dense_up.shape, BF16),
        pltpu.VMEM(w_dense_down.shape, BF16),
        pltpu.VMEM(w_exp_gate.shape[1:], BF16),
        pltpu.VMEM(w_exp_up.shape[1:], BF16),
        pltpu.VMEM((n, units, feats), BF16),
        pltpu.VMEM((n, seqs, wide), BF16),
        pltpu.VMEM((n - 1, seqs, wide), BF16),
        pltpu.VMEM((n, seqs, 128), F32),
        pltpu.VMEM((n - 1, seqs, 128), F32),
        pltpu.VMEM((seqs, wide), F32),
        pltpu.VMEM((n, seqs, hv), BF16),
        pltpu.VMEM((rows, feats), BF16),
        pltpu.VMEM((tn - 1, quarter, feats), BF16),
        pltpu.VMEM((quarter, feats), F32),
        pltpu.VMEM((n, rows, feats), BF16),
        pltpu.VMEM((pieces, 8, 128), F32),
        pltpu.VMEM((n - 1, pieces, 8, 128), F32),
        pltpu.VMEM((tn, pieces, 8, 128), F32),
        pltpu.VMEM((rows, 128), F32),
        pltpu.VMEM((n, seqs, 2 * units), BF16),
        pltpu.VMEM((n - 1, seqs, 2 * units), BF16),
        pltpu.VMEM((n, seqs, units), BF16),
        pltpu.VMEM((rows, 2 * units), F32),
        pltpu.VMEM((n, 2, quarter, feats), BF16),
        pltpu.VMEM((n, quarter, feats), BF16),
        pltpu.VMEM((n - 1, quarter, feats), BF16),
        pltpu.VMEM((quarter, feats), F32),
        pltpu.VMEM((rows, feats), BF16),
        pltpu.VMEM((tn - 1, quarter, feats), BF16),
        pltpu.VMEM((rows, feats), BF16),
        pltpu.VMEM((seqs, hk), F32),
        pltpu.VMEM((128, 128), F32),
        dma((12,)),
        dma((n,)),
        dma((8, n - 1)),
        dma((8, n - 1)),
        dma((4, tn - 1)),
        dma((4, tn - 1)),
        dma((6, n)),
        dma((6, n)),
    ]
    layer_out, new_matrix, new_norm, new_max = pl.pallas_call(
        functools.partial(wide_kernel, n, tn, n * feats),
        out_shape=(
            jax.ShapeDtypeStruct((rows, feats), BF16),
            jax.ShapeDtypeStruct(state_matrix.shape, F32),
            jax.ShapeDtypeStruct((seqs, hk), F32),
            jax.ShapeDtypeStruct((heads, seqs), F32),
        ),
        in_specs=[vmem] * 7 + [hbm] * 12,
        out_specs=(vmem, hbm, vmem, vmem),
        scratch_shapes=scratch,
        compiler_params=pltpu.CompilerParams(
            collective_id=0, has_side_effects=True, vmem_limit_bytes=66_900_000
        ),
    )(
        tokens,
        small,
        w_gates,
        state_norm,
        state_max.T,
        routes.T,
        route_weights.T,
        w_query,
        w_key,
        w_value,
        w_outgate,
        w_mixout,
        state_matrix,
        w_dense_gate,
        w_dense_up,
        w_dense_down,
        w_exp_gate,
        w_exp_up,
        down,
    )
    return (
        layer_out,
        new_matrix,
        new_norm.reshape(seqs, heads, dk),
        new_max.T,
    )


def either(n, tn, tokens, *rest):
    narrow = tokens.shape[1] % 128 == 0 and tokens.shape[0] == 128 and tn == 4 and n == 8
    part = on_device if narrow else wide_on_device
    return part(n, tn, tokens, *rest)


def solution(mesh):
    return jax.shard_map(
        functools.partial(either, mesh.shape["ep"], mesh.shape["tp"]),
        mesh=mesh,
        in_specs=(
            P(None, "ep"),
            P("ep"),
            P("ep", "tp"),
            P("ep", "tp"),
            P("ep", "tp"),
            P("ep", "tp"),
            P("ep", "tp"),
            P("ep", "tp"),
            P("tp"),
            P("tp"),
            P("tp"),
            P("tp", "ep"),
            P("ep", "tp", None, None),
            P("ep", "tp", None),
            P("ep", "tp"),
            P("ep"),
            P("ep"),
            P("ep", "tp"),
            P("ep", "tp"),
            P("tp", "ep"),
            P(),
            P(),
            P("ep", None, "tp"),
            P("ep", None, "tp"),
            P("ep", "tp", None),
        ),
        out_specs=(P(None, "ep"), P("ep", "tp", None, None), P("ep", "tp", None), P("ep", "tp")),
        check_vma=False,
    )
```
